512 devices in a mesh: sp: 64 (over z, y), fs: 4 (over x), tp: 2 (over core).
Axes of the slice: x: 4, y: 8, z: 8, core: 2. Of those that a mesh axis runs over, the one named last changes fastest.
Arguments:
- tokens: bfloat16 [65536, 2048], P('sp'), may hold values from -6 to 6
- norm_gain: float32 [2048], replicated, may hold values from 0.1 to 1.9
- w_query: bfloat16 [2048, 2048], P('sp', ('fs', 'tp')), may hold values from -3.6239223 to 3.6239223
- w_key: bfloat16 [2048, 512], P('sp', ('fs', 'tp')), may hold values from -0.088388348 to 0.088388348
- w_value: bfloat16 [2048, 512], P('sp', ('fs', 'tp')), may hold values from -0.8984375 to 0.8984375
- w_conv_in: bfloat16 [2048, 2048], P('sp', ('fs', 'tp')), may hold values from -0.125 to 0.125
- w_conv_gate: bfloat16 [2048, 2048], P('sp', ('fs', 'tp')), may hold values from -0.125 to 0.125
- conv_taps: bfloat16 [3, 2048], P(None, ('fs', 'tp')), may hold values from -3.5 to 3.5
- sink_logits: float32 [32], P(('fs', 'tp')), may hold values from 2 to 6
Outputs:
- mixed: bfloat16 [65536, 2048], P('sp', ('fs', 'tp'))
- log_sums: float32 [32, 65536], P(('fs', 'tp'), 'sp')
The draws below stay inside these ranges and needn't reach their ends.
All inputs are finite; a program needn't handle non-finite values.
Results may differ from the reference program's by a relative error of at most 0.0077.
Values may be sent and summed in bfloat16 or wider, within the bound.
No kernel may reach another device: no remote copies, remote signals or barrier semaphores. Data moves between devices by JAX's collectives and lax.ppermute only.
A program may use at most 64 MiB of HBM per device.

```python
import math
import jax
import jax.numpy as jnp
from jax import lax

HEAD_DIM = 64
KV_HEADS = 8
GROUP = 4
HEADS = 32
D = 2048
WINDOW = 128
TAPS = 3
TOKENS = 65536


def shared_key_weight(key):
    base_draw = jax.random.normal(jax.random.fold_in(key, 101), (D, KV_HEADS * HEAD_DIM), jnp.float32)
    return jnp.clip(base_draw, -4.0, 4.0) / math.sqrt(D)


def draw_w_key(key, part):
    return shared_key_weight(key).astype(jnp.bfloat16)


def draw_w_query(key, part):
    noise_part = jnp.clip(jax.random.normal(jax.random.fold_in(key, 202), (D, HEADS * HEAD_DIM), jnp.float32), -4.0, 4.0) / math.sqrt(D)
    return noise_part.astype(jnp.bfloat16)


def block_levels(rng, extent, pieces, smallest, largest):
    level, own = 1.0, jax.random.fold_in(rng, 6)
    for position, parts in pieces:
        steps = jnp.exp(jax.random.uniform(jax.random.fold_in(own, position), (parts,), jnp.float32, smallest / len(pieces), largest / len(pieces)))
        level = level * jnp.repeat(steps, extent[position] // parts).reshape([-1 if axis == position else 1 for axis in range(len(extent))])
    return level


def noise(stream_key, extent, width, limit, cuts=(), held_as=jnp.bfloat16):
    result = width * jax.random.normal(stream_key, extent, jnp.float32)
    if cuts:
        result = result * block_levels(stream_key, extent, cuts, -0.22, 0.18)
    return jnp.clip(result, -limit, limit).astype(held_as)


def setup_inputs(seed: int = 0) -> dict:
    keys = jax.random.split(jax.random.key(seed), 10)
    return {
        "tokens": noise(keys[0], (TOKENS, D), 1.0, 6.0, ((0, 64),)),
        "norm_gain": jnp.clip(1.0 + 0.18 * jax.random.normal(keys[1], (D,), jnp.float32), 0.1, 1.9),
        "w_query": draw_w_query(jax.random.fold_in(keys[9], 71), 0),
        "w_key": draw_w_key(jax.random.fold_in(keys[9], 71), 0),
        "w_value": noise(keys[4], (D, KV_HEADS * HEAD_DIM), 0.15, 0.8984375, ((0, 64), (1, 8))),
        "w_conv_in": noise(keys[5], (D, D), D ** -0.5, 0.125, ((0, 64), (1, 8))),
        "w_conv_gate": noise(keys[6], (D, D), D ** -0.5, 0.125, ((0, 64), (1, 8))),
        "conv_taps": noise(keys[7], (TAPS, D), TAPS ** -0.5, 3.5, ((1, 8),)),
        "sink_logits": jnp.clip(2.0 + 4.0 * jax.random.uniform(keys[8], (HEADS,), jnp.float32) ** block_levels(keys[8], (HEADS,), ((0, 8),), -0.2, 0.2), 2.0, 6.0),
    }


EPS = 1e-06

def attend_group(query_blocks, key_span, value_span, sink_group, in_window):
    scores = jnp.einsum('nqgd,nkd->ngqk', query_blocks.astype(jnp.float32), key_span.astype(jnp.float32)) * HEAD_DIM ** (-0.5)
    scores = jnp.where(in_window[:, None], scores, -jnp.inf)
    sink_col = sink_group[None, :, None, None]
    row_top = jnp.maximum(lax.optimization_barrier(jnp.max(scores, axis=-1, keepdims=True)), sink_col)
    raised = jnp.exp(scores - row_top)
    row_sum = lax.optimization_barrier(jnp.sum(raised, axis=-1, keepdims=True)) + jnp.exp(sink_col - row_top)
    soft_weights = (raised / row_sum).astype(jnp.bfloat16)
    attended = jnp.einsum('ngqk,nkd->nqgd', soft_weights.astype(jnp.float32), value_span.astype(jnp.float32))
    return (attended, (row_top + jnp.log(row_sum))[..., 0])

def block_spans(rows_bf, blocks):
    shaped = rows_bf.reshape(blocks, WINDOW, KV_HEADS, HEAD_DIM)
    earlier = jnp.concatenate([jnp.zeros_like(shaped[:1]), shaped[:-1]], axis=0)
    return jnp.concatenate([earlier, shaped], axis=1).transpose(2, 0, 1, 3)

def reference(tokens, norm_gain, w_query, w_key, w_value, w_conv_in, w_conv_gate, conv_taps, sink_logits):
    widened = tokens.astype(jnp.float32)
    normed = (widened * lax.rsqrt(lax.optimization_barrier(jnp.mean(widened * widened, axis=-1, keepdims=True)) + EPS) * norm_gain).astype(jnp.bfloat16)
    query, key_rows, value_rows, conv_in, conv_gate = [jnp.dot(normed, weight, preferred_element_type=jnp.float32).astype(jnp.bfloat16) for weight in (w_query, w_key, w_value, w_conv_in, w_conv_gate)]
    blocks = TOKENS // WINDOW
    query_blocks = query.reshape(blocks, WINDOW, KV_HEADS, GROUP, HEAD_DIM).transpose(2, 0, 1, 3, 4)
    query_idx = jnp.arange(WINDOW)[:, None] + WINDOW
    key_idx = jnp.arange(2 * WINDOW)[None, :]
    offset_gap = query_idx - key_idx
    in_band = (offset_gap >= 0) & (offset_gap < WINDOW)
    block_idx = jnp.arange(blocks)[:, None, None]
    in_window = in_band[None] & ((block_idx > 0) | (key_idx[None] >= WINDOW))
    sink_table = sink_logits.reshape(KV_HEADS, GROUP)
    attended, log_sums = lax.map(lambda group_args: attend_group(group_args[0], group_args[1], group_args[2], group_args[3], in_window), (query_blocks, block_spans(key_rows, blocks), block_spans(value_rows, blocks), sink_table))
    attended = attended.transpose(1, 2, 0, 3, 4).reshape(TOKENS, HEADS * HEAD_DIM)
    log_sums = log_sums.transpose(0, 2, 1, 3).reshape(HEADS, TOKENS)
    padded = jnp.concatenate([jnp.zeros((TAPS - 1, D), jnp.bfloat16), conv_in], axis=0)
    conv_sum = jnp.zeros((TOKENS, D), jnp.float32)
    for tap_idx in range(TAPS):
        conv_sum = conv_sum + conv_taps[tap_idx].astype(jnp.float32) * padded[tap_idx:tap_idx + TOKENS].astype(jnp.float32)
    convolved = conv_gate.astype(jnp.float32) * conv_sum
    mixed = (attended + convolved).astype(jnp.bfloat16)
    return (mixed, log_sums)
```

```python
import jax
import jax.numpy as jnp
from jax import lax
from jax.sharding import Mesh, PartitionSpec as P

HEAD_DIM = 64
WINDOW = 128
TAPS = 3
EPS = 1e-06

SP = ("zh", "zl", "yh", "yl")
COLS = ("fs", "tp")
SIDE = 8


def shift(value, dz, dy):
    pairs = []
    for z in range(SIDE):
        for y in range(SIDE):
            pairs.append((z * SIDE + y, (z + dz) % SIDE * SIDE + (y + dy) % SIDE))
    return lax.ppermute(value, SP, pairs)


def passed_along(value):
    n = SIDE * SIDE
    return lax.ppermute(value, SP, [(i, i + 1) for i in range(n - 1)])


def block_spans(earlier_rows, current_rows, blocks, kv_local):
    joined = jnp.concatenate([earlier_rows, current_rows], axis=0).reshape(
        blocks + 1, WINDOW, kv_local, HEAD_DIM
    )
    return jnp.concatenate([joined[:-1], joined[1:]], axis=1)


def body(
    tokens, norm_gain, w_query, w_key, w_value, w_conv_in, w_conv_gate, conv_taps, sink_logits
):
    tok_rows, width = tokens.shape
    shard_rows = w_key.shape[0]
    mine = jnp.concatenate([w_key, w_value, w_query, w_conv_in, w_conv_gate], axis=1)
    cols = mine.shape[1]
    own = lax.all_to_all(jnp.broadcast_to(mine[None], (16,) + mine.shape), ("zh", "yh"), 0, 0)
    own = own.reshape(16 * shard_rows, cols)
    from_y = shift(own, 0, 1)
    from_z = shift(own, 1, 0)
    from_d = shift(own, -1, -1)

    widened = tokens.astype(jnp.float32)
    normed = (
        widened * lax.rsqrt(jnp.mean(widened * widened, axis=-1, keepdims=True) + EPS) * norm_gain
    ).astype(jnp.bfloat16)
    span = SIDE * shard_rows
    src = jnp.arange(span)
    dst = (src // shard_rows) % 2 * (span // 2) + src // (2 * shard_rows) * shard_rows + src % shard_rows
    swap = (dst[:, None] == jnp.arange(span)[None, :]).astype(jnp.bfloat16)
    mixed_cols = jnp.dot(
        normed.reshape(tok_rows * SIDE, span), swap, preferred_element_type=jnp.float32
    ).astype(jnp.bfloat16)
    classes = (
        mixed_cols.reshape(tok_rows, 4, 2, 2, span // 2)
        .transpose(2, 3, 0, 1, 4)
        .reshape(4, tok_rows, width // 4)
    )
    pz, py = lax.axis_index("zl"), lax.axis_index("yl")

    def part(rz, ry, weights):
        x = lax.dynamic_index_in_dim(classes, (pz ^ rz) * 2 + (py ^ ry), 0, keepdims=False)
        return jnp.dot(x, weights, preferred_element_type=jnp.float32)

    out = part(0, 0, own) + part(0, 1, from_y) + part(1, 0, from_z) + part(1, 1, from_d)
    out = out.astype(jnp.bfloat16)
    kw, qw, cw = w_key.shape[1], w_query.shape[1], w_conv_in.shape[1]
    key_rows, value_rows, query, conv_in, conv_gate = jnp.split(
        out, [kw, 2 * kw, 2 * kw + qw, 2 * kw + qw + cw], axis=1
    )
    rim_rows = TAPS - 1
    both_prev = passed_along(out[tok_rows - WINDOW :, : 2 * kw])
    key_prev, value_prev = both_prev[:, :kw], both_prev[:, kw:]
    conv_prev = passed_along(conv_in[tok_rows - rim_rows :])
    kv_local = kw // HEAD_DIM
    group_size = qw // kw
    blocks = tok_rows // WINDOW
    offset = lax.axis_index(SP) * tok_rows
    query_blocks = query.reshape(blocks, WINDOW, kv_local, group_size, HEAD_DIM)
    key_span = block_spans(key_prev, key_rows, blocks, kv_local)
    value_span = block_spans(value_prev, value_rows, blocks, kv_local)
    scores = jnp.einsum(
        "nqhgd,nkhd->nhgqk", query_blocks, key_span, preferred_element_type=jnp.float32
    ) * HEAD_DIM ** (-0.5)
    block_base = offset + WINDOW * jnp.arange(blocks)[:, None, None]
    query_idx = jnp.arange(WINDOW)[None, :, None]
    key_idx = jnp.arange(2 * WINDOW)[None, None, :]
    offset_gap = query_idx + WINDOW - key_idx
    in_window = (offset_gap >= 0) & (offset_gap < WINDOW) & (block_base - WINDOW + key_idx >= 0)
    scores = jnp.where(in_window[:, None, None], scores, -jnp.inf)
    sink_col = sink_logits.reshape(kv_local, group_size)[None, :, :, None, None]
    row_top = jnp.maximum(jnp.max(scores, axis=-1, keepdims=True), sink_col)
    raised = jnp.exp(scores - row_top)
    row_sum = jnp.sum(raised, axis=-1, keepdims=True) + jnp.exp(sink_col - row_top)
    soft_weights = (raised / row_sum).astype(jnp.bfloat16)
    attended = jnp.einsum(
        "nhgqk,nkhd->nqhgd", soft_weights, value_span, preferred_element_type=jnp.float32
    ).reshape(tok_rows, kv_local * group_size * HEAD_DIM)
    log_sums = (
        (row_top + jnp.log(row_sum))[..., 0]
        .transpose(1, 2, 0, 3)
        .reshape(kv_local * group_size, tok_rows)
    )
    padded = jnp.concatenate([conv_prev, conv_in], axis=0)
    conv_sum = jnp.zeros((tok_rows, cw), jnp.float32)
    for tap_idx in range(TAPS):
        conv_sum = conv_sum + conv_taps[tap_idx].astype(jnp.float32) * padded[
            tap_idx : tap_idx + tok_rows
        ].astype(jnp.float32)
    convolved = conv_gate.astype(jnp.float32) * conv_sum
    mixed = (attended + convolved).astype(jnp.bfloat16)
    return (mixed, log_sums)


def solution(mesh):
    fine = Mesh(
        mesh.devices.reshape(4, 2, 4, 2, mesh.shape["fs"], mesh.shape["tp"]), SP + COLS
    )
    weights = P(SP, COLS)
    return jax.shard_map(
        body,
        mesh=fine,
        in_specs=(P(SP, None), P()) + (weights,) * 5 + (P(None, COLS), P(COLS)),
        out_specs=(P(SP, COLS), P(COLS, SP)),
        check_vma=False,
    )
```

```python
import jax
import jax.numpy as jnp
from jax import lax
from jax.experimental import pallas as pl
from jax.experimental.pallas import tpu as pltpu
from jax.sharding import Mesh, PartitionSpec as P


HEAD_DIM = 64
WINDOW = 128
EPS = 1e-06

SP = ("zh", "zl", "yh", "yl")
COLS = ("fs", "tp")
SIDE = 8
LANES = 128


def shift(value, dz, dy):
    pairs = []
    for z in range(SIDE):
        for y in range(SIDE):
            pairs.append((z * SIDE + y, (z + dz) % SIDE * SIDE + (y + dy) % SIDE))
    return lax.ppermute(value, SP, pairs)


def passed_along(value):
    n = SIDE * SIDE
    return lax.ppermute(value, SP, [(i, i + 1) for i in range(n - 1)])


def settings(mib):
    return pltpu.CompilerParams(vmem_limit_bytes=mib << 20)


def cost(us):
    return pl.CostEstimate(flops=int(us * 3.9e6), bytes_accessed=1 << 20, transcendentals=0)


def dot(a, b, dims=((1,), (0,))):
    return lax.dot_general(a, b, (dims, ((), ())), preferred_element_type=jnp.float32)


def norm_kernel(place, tok_ref, gain_ref, out_ref):
    widened = tok_ref[...].astype(jnp.float32)
    scale = lax.rsqrt(jnp.mean(widened * widened, axis=-1, keepdims=True) + EPS)
    normed = (widened * scale * gain_ref[...]).astype(jnp.bfloat16)
    span = 2 * LANES
    row = lax.broadcasted_iota(jnp.int32, (span, span), 0)
    col = lax.broadcasted_iota(jnp.int32, (span, span), 1)
    target = ((row >> 5) & 1) * LANES + (row >> 6) * 32 + (row & 31)
    swap = (target == col).astype(jnp.bfloat16)
    for zh in range(4):
        for zl in range(2):
            at = (zh * 2 + zl) * span
            sorted_cols = dot(normed[:, at : at + span], swap).astype(jnp.bfloat16)
            for yl in range(2):
                out_ref[(place[0] ^ zl) * 2 + (place[1] ^ yl), :, zh * LANES : (zh + 1) * LANES] = (
                    sorted_cols[:, yl * LANES : (yl + 1) * LANES]
                )


def norm_classes(place, rows, gain, block):
    n, width = rows.shape
    return pl.pallas_call(
        norm_kernel,
        grid_spec=pltpu.PrefetchScalarGridSpec(
            num_scalar_prefetch=1,
            grid=(n // block,),
            in_specs=[
                pl.BlockSpec((block, width), lambda i, p: (i, 0)),
                pl.BlockSpec((1, width), lambda i, p: (0, 0)),
            ],
            out_specs=pl.BlockSpec((4, block, width // 4), lambda i, p: (0, i, 0)),
        ),
        out_shape=jax.ShapeDtypeStruct((4, n, width // 4), jnp.bfloat16),
        compiler_params=settings(14),
        cost_estimate=cost(5 if n > 16 else 1),
        name="norm",
    )(place, rows, gain)


def attend_block(q, kv_prev, kv_cur, sinks, has_prev):
    lane = lax.broadcasted_iota(jnp.int32, (WINDOW, LANES), 1)
    left = lane < HEAD_DIM

    def split(kv):
        swapped = pltpu.roll(kv.astype(jnp.float32), HEAD_DIM, 1).astype(jnp.bfloat16)
        zero = jnp.zeros_like(kv)
        return jnp.where(left, kv, zero), jnp.where(left, zero, swapped)

    prev_lo, prev_hi = split(kv_prev)
    cur_lo, cur_hi = split(kv_cur)
    keys = jnp.concatenate([prev_lo, cur_lo, prev_hi, cur_hi], axis=0)
    key_idx = lax.broadcasted_iota(jnp.int32, (WINDOW, WINDOW), 0)
    query_idx = lax.broadcasted_iota(jnp.int32, (WINDOW, WINDOW), 1)
    from_prev = key_idx > query_idx
    weights, logs = [], []
    for pair in range(2):
        both = dot(keys, q[:, pair * LANES : (pair + 1) * LANES], ((1,), (1,)))
        for side in range(2):
            head = pair * 2 + side
            prev = both[side * 256 : side * 256 + WINDOW]
            cur = both[side * 256 + WINDOW : side * 256 + 2 * WINDOW]
            if has_prev is not None:
                prev = jnp.where(has_prev, prev, -jnp.inf)
            scores = jnp.where(from_prev, prev, cur) * HEAD_DIM ** (-0.5)
            top = jnp.maximum(jnp.max(scores, axis=0, keepdims=True), sinks[head])
            raised = jnp.exp(scores - top)
            total = jnp.sum(raised, axis=0, keepdims=True) + jnp.exp(sinks[head] - top)
            logs.append(top + jnp.log(total))
            share = raised / total
            zero = jnp.zeros_like(share)
            weights.append(
                jnp.concatenate(
                    [jnp.where(from_prev, share, zero), jnp.where(from_prev, zero, share)], axis=0
                ).astype(jnp.bfloat16)
            )
    values = jnp.concatenate([kv_prev, kv_cur], axis=0)
    outs = []
    for pair in range(2):
        got = dot(values, jnp.concatenate(weights[pair * 2 : pair * 2 + 2], axis=1), ((0,), (0,)))
        stacked = jnp.concatenate([got[HEAD_DIM:, :WINDOW], got[HEAD_DIM:, WINDOW:]], axis=0)
        outs.append(stacked.T)
    return jnp.concatenate(outs, axis=1), jnp.concatenate(logs, axis=0)


def tail_kernel(x_ref, w0, w1, w2, w3, out_ref):
    acc = dot(x_ref[0], w0[...])
    for c, w in ((1, w1), (2, w2), (3, w3)):
        acc = acc + dot(x_ref[c], w[...])
    out_ref[...] = acc.astype(jnp.bfloat16)


def tail_rows(x, parts):
    n, depth = x.shape[1], x.shape[2]
    last = n // WINDOW - 1
    return pl.pallas_call(
        tail_kernel,
        grid=(1,),
        in_specs=[pl.BlockSpec((4, WINDOW, depth), lambda i: (0, last, 0))]
        + [pl.BlockSpec((depth, LANES), lambda i: (0, 0))] * 4,
        out_specs=pl.BlockSpec((WINDOW, LANES), lambda i: (0, 0)),
        out_shape=jax.ShapeDtypeStruct((WINDOW, LANES), jnp.bfloat16),
        compiler_params=settings(6),
        cost_estimate=cost(1),
        name="tail",
    )(x, *parts)


def attn_kernel(sinks, x_ref, w0, w1, w2, w3, att_ref, log_ref, rows_ref):
    n = x_ref.shape[1]
    step = 256
    parts = (w0, w1, w2, w3)
    for at in range(0, n, step):
        acc = dot(x_ref[0, at : at + step, :], w0[...])
        for c in range(1, 4):
            acc = acc + dot(x_ref[c, at : at + step, :], parts[c][...])
        rows_ref[at : at + step, :] = acc.astype(jnp.bfloat16)
    heads = [sinks[h] for h in range(4)]
    att_ref[:WINDOW, :] = jnp.zeros((WINDOW, 2 * LANES), jnp.float32)
    log_ref[:, :WINDOW] = jnp.zeros((4, WINDOW), jnp.float32)

    for b in range(1, n // WINDOW):
        here, before = b * WINDOW, (b - 1) * WINDOW
        att, logs = attend_block(
            rows_ref[here : here + WINDOW, LANES:],
            rows_ref[before : before + WINDOW, :LANES],
            rows_ref[here : here + WINDOW, :LANES],
            heads,
            None,
        )
        att_ref[here : here + WINDOW, :] = att
        log_ref[:, here : here + WINDOW] = logs


VMEM = pl.BlockSpec(memory_space=pltpu.VMEM)
SMEM = pl.BlockSpec(memory_space=pltpu.SMEM)


def attention(sinks, x, parts):
    n = x.shape[1]
    cols = parts[0].shape[1]
    return pl.pallas_call(
        attn_kernel,
        in_specs=[SMEM] + [VMEM] * 5,
        out_specs=[VMEM] * 3,
        out_shape=[
            jax.ShapeDtypeStruct((n, 2 * LANES), jnp.float32),
            jax.ShapeDtypeStruct((4, n), jnp.float32),
            jax.ShapeDtypeStruct((n, cols), jnp.bfloat16),
        ],
        compiler_params=settings(20),
        cost_estimate=cost(8),
        name="attn",
    )(sinks, x, *parts)


def conv_kernel(
    sinks, has_prev, x_ref, w0, w1, w2, w3, prev_x, taps_ref, att_ref, log_ref, rows_ref, halo_ref,
    out_ref, log_out, pad_ref,
):
    n = x_ref.shape[1]
    width = 2 * LANES
    step = 256
    parts = (w0, w1, w2, w3)
    acc = dot(prev_x[0], w0[:, :width])
    for c in range(1, 4):
        acc = acc + dot(prev_x[c], parts[c][:, :width])
    pad_ref[:8, :] = acc[8:16].astype(jnp.bfloat16).astype(jnp.float32)
    att0, log0 = attend_block(
        rows_ref[:WINDOW, LANES:],
        halo_ref[...],
        rows_ref[:WINDOW, :LANES],
        [sinks[h] for h in range(4)],
        has_prev[0] > 0,
    )
    log_out[...] = log_ref[...]
    log_out[:, :WINDOW] = log0
    taps = taps_ref[...].astype(jnp.float32)
    for at in range(0, n, step):
        acc = dot(x_ref[0, at : at + step, :], w0[...])
        for c in range(1, 4):
            acc = acc + dot(x_ref[c, at : at + step, :], parts[c][...])
        rounded = acc.astype(jnp.bfloat16).astype(jnp.float32)
        pad_ref[8 + at : 8 + at + step, :] = rounded[:, :width]
        total = taps[0:1] * pad_ref[6 + at : 6 + at + step, :]
        total = total + taps[1:2] * pad_ref[7 + at : 7 + at + step, :]
        total = total + taps[2:3] * rounded[:, :width]
        gated = rounded[:, width:] * total
        if at == 0:
            first = jnp.concatenate([att0, att_ref[WINDOW:step, :]], axis=0)
        else:
            first = att_ref[at : at + step, :]
        out_ref[at : at + step, :] = (first + gated).astype(jnp.bfloat16)


def convolution(sinks, has_prev, x, parts, prev_x, taps, att, logs, rows, halo):
    n = x.shape[1]
    return pl.pallas_call(
        conv_kernel,
        in_specs=[SMEM] * 2 + [VMEM] * 11,
        out_specs=[VMEM] * 2,
        out_shape=[
            jax.ShapeDtypeStruct((n, 2 * LANES), jnp.bfloat16),
            jax.ShapeDtypeStruct((4, n), jnp.float32),
        ],
        scratch_shapes=[pltpu.VMEM((n + 8, 2 * LANES), jnp.float32)],
        compiler_params=settings(20),
        cost_estimate=cost(6),
        name="conv",
    )(sinks, has_prev, x, *parts, prev_x, taps, att, logs, rows, halo)


def body(
    tokens, norm_gain, w_query, w_key, w_value, w_conv_in, w_conv_gate, conv_taps, sink_logits
):
    return layer(
        tokens, norm_gain, (w_key, w_value, w_query), (w_conv_in, w_conv_gate), conv_taps, sink_logits
    )


def layer(tokens, norm_gain, attn_weights, conv_weights, conv_taps, sink_logits):
    n, width = tokens.shape
    mine = jnp.concatenate(attn_weights + conv_weights, axis=1)
    cut = sum(w.shape[1] for w in attn_weights)
    sent = jnp.broadcast_to(mine[None], (16,) + mine.shape)
    own = lax.all_to_all(sent, ("zh", "yh"), 0, 0)
    own = own.reshape(16 * mine.shape[0], mine.shape[1])
    prev_tokens = passed_along(tokens[n - 16 :])

    place = jnp.stack([lax.axis_index("zl"), lax.axis_index("yl")]).astype(jnp.int32)
    gain = norm_gain.reshape(1, width)
    x = norm_classes(place, tokens, gain, 256)
    prev_x = norm_classes(place, prev_tokens, gain, 16)

    def classes(block):
        parts = [block]
        for dz, dy in ((0, 1), (1, 0), (-1, -1)):
            parts.append(shift(block, dz, dy))
        return parts

    parts_a = classes(own[:, :cut])
    parts_b = classes(own[:, cut:])
    has_prev = (lax.axis_index(SP) > 0).astype(jnp.int32).reshape(1)
    last = tail_rows(x, parts_a)
    halo = passed_along(last)
    att, logs, rows = attention(sink_logits, x, parts_a)
    return tuple(
        convolution(
            sink_logits, has_prev, x, parts_b, prev_x, conv_taps, att, logs, rows, halo
        )
    )


def solution(mesh):
    fine = Mesh(
        mesh.devices.reshape(4, 2, 4, 2, mesh.shape["fs"], mesh.shape["tp"]), SP + COLS
    )
    weights = P(SP, COLS)
    return jax.shard_map(
        body,
        mesh=fine,
        in_specs=(P(SP, None), P()) + (weights,) * 5 + (P(None, COLS), P(COLS)),
        out_specs=(P(SP, COLS), P(COLS, SP)),
        check_vma=False,
    )
```

```python
import functools

import jax
import jax.numpy as jnp
from jax import lax
from jax.experimental import pallas as pl
from jax.experimental.pallas import tpu as pltpu
from jax.sharding import Mesh, PartitionSpec as P


HEAD_DIM = 64
WINDOW = 128
EPS = 1e-06

SP = ("zh", "zl", "yh", "yl")
COLS = ("fs", "tp")
SIDE = 8
LANES = 128
VMEM = pl.BlockSpec(memory_space=pltpu.VMEM)
SMEM = pl.BlockSpec(memory_space=pltpu.SMEM)
HBM = pl.BlockSpec(memory_space=pltpu.HBM)


def shift(value, dz, dy):
    pairs = []
    for z in range(SIDE):
        for y in range(SIDE):
            pairs.append((z * SIDE + y, (z + dz) % SIDE * SIDE + (y + dy) % SIDE))
    return lax.ppermute(value, SP, pairs)


def passed_along(value):
    n = SIDE * SIDE
    return lax.ppermute(value, SP, [(i, i + 1) for i in range(n - 1)])


def settings(mib):
    return pltpu.CompilerParams(vmem_limit_bytes=mib << 20)


def cost(us):
    return pl.CostEstimate(flops=int(us * 3.9e6), bytes_accessed=1 << 20, transcendentals=0)


def dot(a, b, dims=((1,), (0,))):
    return lax.dot_general(a, b, (dims, ((), ())), preferred_element_type=jnp.float32)


def norm_kernel(place, tok_hbm, gain_ref, out_hbm, *, block):
    n, width = tok_hbm.shape
    span = 2 * LANES
    row = lax.broadcasted_iota(jnp.int32, (span, span), 0)
    col = lax.broadcasted_iota(jnp.int32, (span, span), 1)
    target = ((row >> 5) & 1) * LANES + (row >> 6) * 32 + (row & 31)
    swap = (target == col).astype(jnp.bfloat16)

    def step(tok_ref, out_ref):
        widened = tok_ref[...].astype(jnp.float32)
        scale = lax.rsqrt(jnp.mean(widened * widened, axis=-1, keepdims=True) + EPS)
        normed = (widened * scale * gain_ref[...]).astype(jnp.bfloat16)
        for zh in range(4):
            for zl in range(2):
                at = (zh * 2 + zl) * span
                sorted_cols = dot(normed[:, at : at + span], swap).astype(jnp.bfloat16)
                for yl in range(2):
                    into = (place[0] ^ zl) * 2 + (place[1] ^ yl)
                    out_ref[into, :, zh * LANES : (zh + 1) * LANES] = sorted_cols[
                        :, yl * LANES : (yl + 1) * LANES
                    ]

    pltpu.emit_pipeline(
        step,
        grid=(n // block,),
        in_specs=[pl.BlockSpec((block, width), lambda i: (i, 0))],
        out_specs=[pl.BlockSpec((4, block, width // 4), lambda i: (0, i, 0))],
    )(tok_hbm, out_hbm)


def norm_classes(place, rows, gain, block):
    n, width = rows.shape
    return pl.pallas_call(
        functools.partial(norm_kernel, block=block),
        in_specs=[SMEM, HBM, VMEM],
        out_specs=HBM,
        out_shape=pltpu.HBM((4, n, width // 4), jnp.bfloat16),
        compiler_params=settings(14),
        cost_estimate=cost(5 if n > 16 else 1),
        name="norm",
    )(place, rows, gain)


def attend_block(q, kv_prev, kv_cur, sinks, has_prev):
    lane = lax.broadcasted_iota(jnp.int32, (WINDOW, LANES), 1)
    left = lane < HEAD_DIM

    def split(kv):
        swapped = pltpu.roll(kv.astype(jnp.float32), HEAD_DIM, 1).astype(jnp.bfloat16)
        zero = jnp.zeros_like(kv)
        return jnp.where(left, kv, zero), jnp.where(left, zero, swapped)

    prev_lo, prev_hi = split(kv_prev)
    cur_lo, cur_hi = split(kv_cur)
    keys = jnp.concatenate([prev_lo, cur_lo, prev_hi, cur_hi], axis=0)
    key_idx = lax.broadcasted_iota(jnp.int32, (WINDOW, WINDOW), 0)
    query_idx = lax.broadcasted_iota(jnp.int32, (WINDOW, WINDOW), 1)
    from_prev = key_idx > query_idx
    weights, logs = [], []
    for pair in range(2):
        both = dot(keys, q[:, pair * LANES : (pair + 1) * LANES], ((1,), (1,)))
        for side in range(2):
            head = pair * 2 + side
            prev = both[side * 256 : side * 256 + WINDOW]
            cur = both[side * 256 + WINDOW : side * 256 + 2 * WINDOW]
            if has_prev is not None:
                prev = jnp.where(has_prev, prev, -jnp.inf)
            scores = jnp.where(from_prev, prev, cur) * HEAD_DIM ** (-0.5)
            top = jnp.maximum(jnp.max(scores, axis=0, keepdims=True), sinks[head])
            raised = jnp.exp(scores - top)
            total = jnp.sum(raised, axis=0, keepdims=True) + jnp.exp(sinks[head] - top)
            logs.append(top + jnp.log(total))
            share = raised / total
            zero = jnp.zeros_like(share)
            weights.append(
                jnp.concatenate(
                    [jnp.where(from_prev, share, zero), jnp.where(from_prev, zero, share)], axis=0
                ).astype(jnp.bfloat16)
            )
    values = jnp.concatenate([kv_prev, kv_cur], axis=0)
    outs = []
    for pair in range(2):
        got = dot(values, jnp.concatenate(weights[pair * 2 : pair * 2 + 2], axis=1), ((0,), (0,)))
        stacked = jnp.concatenate([got[HEAD_DIM:, :WINDOW], got[HEAD_DIM:, WINDOW:]], axis=0)
        outs.append(stacked.T)
    return jnp.concatenate(outs, axis=1), jnp.concatenate(logs, axis=0)


def tail_kernel(x_hbm, w0, w1, w2, w3, out_ref, x_ref, sem):
    n = x_hbm.shape[1]
    copy = pltpu.make_async_copy(x_hbm.at[:, n - WINDOW : n, :], x_ref, sem)
    copy.start()
    copy.wait()
    acc = dot(x_ref[0], w0[:, :LANES])
    for c, w in ((1, w1), (2, w2), (3, w3)):
        acc = acc + dot(x_ref[c], w[:, :LANES])
    out_ref[...] = acc.astype(jnp.bfloat16)


def tail_rows(x, parts):
    return pl.pallas_call(
        tail_kernel,
        in_specs=[HBM] + [VMEM] * 4,
        out_specs=VMEM,
        out_shape=jax.ShapeDtypeStruct((WINDOW, LANES), jnp.bfloat16),
        scratch_shapes=[
            pltpu.VMEM((4, WINDOW, x.shape[2]), jnp.bfloat16),
            pltpu.SemaphoreType.DMA(()),
        ],
        compiler_params=settings(6),
        cost_estimate=cost(1),
        name="tail",
    )(x, *parts)


def attn_kernel(sinks, x_hbm, w0, w1, w2, w3, att_ref, log_ref, rows_ref, x_ref, sems):
    n = x_ref.shape[1]
    step = 256
    parts = (w0, w1, w2, w3)
    copies = []
    for k, at in enumerate(range(0, n, step)):
        copies.append(
            pltpu.make_async_copy(
                x_hbm.at[:, at : at + step, :], x_ref.at[:, at : at + step, :], sems.at[k]
            )
        )
        copies[-1].start()
    for k, at in enumerate(range(0, n, step)):
        copies[k].wait()
        acc = dot(x_ref[0, at : at + step, :], w0[...])
        for c in range(1, 4):
            acc = acc + dot(x_ref[c, at : at + step, :], parts[c][...])
        rows_ref[at : at + step, :] = acc.astype(jnp.bfloat16)
    heads = [sinks[h] for h in range(4)]
    att_ref[:WINDOW, :] = jnp.zeros((WINDOW, 2 * LANES), jnp.float32)
    log_ref[:, :WINDOW] = jnp.zeros((4, WINDOW), jnp.float32)

    for b in range(1, n // WINDOW):
        here, before = b * WINDOW, (b - 1) * WINDOW
        att, logs = attend_block(
            rows_ref[here : here + WINDOW, LANES:],
            rows_ref[before : before + WINDOW, :LANES],
            rows_ref[here : here + WINDOW, :LANES],
            heads,
            None,
        )
        att_ref[here : here + WINDOW, :] = att
        log_ref[:, here : here + WINDOW] = logs


def attention(sinks, x, parts):
    n = x.shape[1]
    cols = parts[0].shape[1]
    return pl.pallas_call(
        attn_kernel,
        in_specs=[SMEM, HBM] + [VMEM] * 4,
        out_specs=[VMEM] * 4,
        out_shape=[
            jax.ShapeDtypeStruct((n, 2 * LANES), jnp.float32),
            jax.ShapeDtypeStruct((4, n), jnp.float32),
            jax.ShapeDtypeStruct((n, cols), jnp.bfloat16),
            jax.ShapeDtypeStruct(x.shape, x.dtype),
        ],
        scratch_shapes=[pltpu.SemaphoreType.DMA((n // 256,))],
        compiler_params=settings(20),
        cost_estimate=cost(8),
        name="attn",
    )(sinks, x, *parts)


def conv_kernel(
    sinks, place, x_ref, w0, w1, w2, w3, prev_x, taps_ref, att_ref, log_ref, rows_ref, halo_ref,
    out_ref, log_out, pad_ref,
):
    n = x_ref.shape[1]
    width = 2 * LANES
    step = 256
    parts = (w0, w1, w2, w3)
    acc = dot(prev_x[0], w0[:, :width])
    for c in range(1, 4):
        acc = acc + dot(prev_x[c], parts[c][:, :width])
    pad_ref[:8, :] = acc[8:16].astype(jnp.bfloat16).astype(jnp.float32)
    att0, log0 = attend_block(
        rows_ref[:WINDOW, LANES:],
        halo_ref[...],
        rows_ref[:WINDOW, :LANES],
        [sinks[h] for h in range(4)],
        place[2] > 0,
    )
    log_out[...] = log_ref[...]
    log_out[:, :WINDOW] = log0
    taps = taps_ref[...].astype(jnp.float32)
    for at in range(0, n, step):
        acc = dot(x_ref[0, at : at + step, :], w0[...])
        for c in range(1, 4):
            acc = acc + dot(x_ref[c, at : at + step, :], parts[c][...])
        rounded = acc.astype(jnp.bfloat16).astype(jnp.float32)
        pad_ref[8 + at : 8 + at + step, :] = rounded[:, :width]
        total = taps[0:1] * pad_ref[6 + at : 6 + at + step, :]
        total = total + taps[1:2] * pad_ref[7 + at : 7 + at + step, :]
        total = total + taps[2:3] * rounded[:, :width]
        gated = rounded[:, width:] * total
        if at == 0:
            first = jnp.concatenate([att0, att_ref[WINDOW:step, :]], axis=0)
        else:
            first = att_ref[at : at + step, :]
        out_ref[at : at + step, :] = (first + gated).astype(jnp.bfloat16)


def convolution(sinks, place, x, parts, prev_x, taps, att, logs, rows, halo):
    n = x.shape[1]
    return pl.pallas_call(
        conv_kernel,
        in_specs=[SMEM] * 2 + [VMEM] * 11,
        out_specs=[VMEM] * 2,
        out_shape=[
            jax.ShapeDtypeStruct((n, 2 * LANES), jnp.bfloat16),
            jax.ShapeDtypeStruct((4, n), jnp.float32),
        ],
        scratch_shapes=[pltpu.VMEM((n + 8, 2 * LANES), jnp.float32)],
        compiler_params=settings(20),
        cost_estimate=cost(6),
        name="conv",
    )(sinks, place, x, *parts, prev_x, taps, att, logs, rows, halo)


def body(
    tokens, norm_gain, w_query, w_key, w_value, w_conv_in, w_conv_gate, conv_taps, sink_logits
):
    return layer(
        tokens, norm_gain, (w_key, w_value, w_query), (w_conv_in, w_conv_gate), conv_taps, sink_logits
    )


def layer(tokens, norm_gain, attn_weights, conv_weights, conv_taps, sink_logits):
    n, width = tokens.shape
    gain = norm_gain.reshape(1, width)
    place = jnp.stack(
        [lax.axis_index("zl"), lax.axis_index("yl"), jnp.minimum(lax.axis_index(SP), 1)]
    ).astype(jnp.int32)

    def gathered(weights):
        mine = jnp.concatenate(weights, axis=1)
        sent = jnp.broadcast_to(mine[None], (16,) + mine.shape)
        own = lax.all_to_all(sent, ("zh", "yh"), 0, 0)
        return own.reshape(16 * mine.shape[0], mine.shape[1])

    def classes(block):
        parts = [block]
        for dz, dy in ((0, 1), (1, 0), (-1, -1)):
            parts.append(shift(block, dz, dy))
        return parts

    own_a = gathered(attn_weights)
    own_b = gathered(conv_weights)
    prev_tokens = passed_along(tokens[n - 16 :])
    x = norm_classes(place, pltpu.with_memory_space_constraint(tokens, pltpu.HBM), gain, 256)
    x = pltpu.with_memory_space_constraint(x, pltpu.HBM)
    prev_x = norm_classes(place, prev_tokens, gain, 16)
    parts_a = classes(own_a)
    parts_b = classes(own_b)
    last = tail_rows(x, parts_a)
    halo = passed_along(last)
    att, logs, rows, x_near = attention(sink_logits, x, parts_a)
    return tuple(
        convolution(sink_logits, place, x_near, parts_b, prev_x, conv_taps, att, logs, rows, halo)
    )


def solution(mesh):
    fine = Mesh(
        mesh.devices.reshape(4, 2, 4, 2, mesh.shape["fs"], mesh.shape["tp"]), SP + COLS
    )
    weights = P(SP, COLS)
    return jax.shard_map(
        body,
        mesh=fine,
        in_specs=(P(SP, None), P()) + (weights,) * 5 + (P(None, COLS), P(COLS)),
        out_specs=(P(SP, COLS), P(COLS, SP)),
        check_vma=False,
    )
```

```python
import jax
import jax.numpy as jnp
from jax import lax
from jax.experimental import pallas as pl
from jax.experimental.pallas import tpu as pltpu
from jax.sharding import Mesh, PartitionSpec as P


HEAD_DIM = 64
WINDOW = 128
EPS = 1e-06

SP = ("zh", "zl", "yh", "yl")
COLS = ("fs", "tp")
SIDE = 8
LANES = 128
RIM = 16
VMEM = pl.BlockSpec(memory_space=pltpu.VMEM)
SMEM = pl.BlockSpec(memory_space=pltpu.SMEM)
HBM = pl.BlockSpec(memory_space=pltpu.HBM)


def shift(value, dz, dy):
    pairs = []
    for z in range(SIDE):
        for y in range(SIDE):
            pairs.append((z * SIDE + y, (z + dz) % SIDE * SIDE + (y + dy) % SIDE))
    return lax.ppermute(value, SP, pairs)


def passed_along(value):
    n = SIDE * SIDE
    return lax.ppermute(value, SP, [(i, i + 1) for i in range(n - 1)])


def settings(mib):
    return pltpu.CompilerParams(vmem_limit_bytes=mib << 20)


def cost(us):
    return pl.CostEstimate(flops=int(us * 3.9e6), bytes_accessed=1 << 20, transcendentals=0)


def dot(a, b, dims=((1,), (0,))):
    return lax.dot_general(a, b, (dims, ((), ())), preferred_element_type=jnp.float32)


def column_sort():
    span = 2 * LANES
    row = lax.broadcasted_iota(jnp.int32, (span, span), 0)
    col = lax.broadcasted_iota(jnp.int32, (span, span), 1)
    target = ((row >> 5) & 1) * LANES + (row >> 6) * 32 + (row & 31)
    return (target == col).astype(jnp.bfloat16)


def norm_into(place, rows, gain, swap, out_ref):
    widened = rows.astype(jnp.float32)
    scale = lax.rsqrt(jnp.mean(widened * widened, axis=-1, keepdims=True) + EPS)
    normed = (widened * scale * gain).astype(jnp.bfloat16)
    span = 2 * LANES
    for zh in range(4):
        for zl in range(2):
            at = (zh * 2 + zl) * span
            sorted_cols = dot(normed[:, at : at + span], swap).astype(jnp.bfloat16)
            for yl in range(2):
                into = (place[0] ^ zl) * 2 + (place[1] ^ yl)
                out_ref[into, :, zh * LANES : (zh + 1) * LANES] = sorted_cols[
                    :, yl * LANES : (yl + 1) * LANES
                ]


def norm_kernel(place, tok_ref, gain_ref, out_ref):
    norm_into(place, tok_ref[...], gain_ref[...], column_sort(), out_ref)


def norm_classes(place, rows, gain, block):
    n, width = rows.shape
    return pl.pallas_call(
        norm_kernel,
        grid_spec=pltpu.PrefetchScalarGridSpec(
            num_scalar_prefetch=1,
            grid=(n // block,),
            in_specs=[
                pl.BlockSpec((block, width), lambda i, p: (i, 0)),
                pl.BlockSpec((1, width), lambda i, p: (0, 0)),
            ],
            out_specs=pl.BlockSpec((4, block, width // 4), lambda i, p: (0, i, 0)),
        ),
        out_shape=jax.ShapeDtypeStruct((4, n, width // 4), jnp.bfloat16),
        compiler_params=settings(14),
        cost_estimate=cost(5),
        name="norm",
    )(place, rows, gain)


def attend_block(q, kv_prev, kv_cur, sinks, has_prev):
    lane = lax.broadcasted_iota(jnp.int32, (WINDOW, LANES), 1)
    left = lane < HEAD_DIM

    def split(kv):
        swapped = pltpu.roll(kv.astype(jnp.float32), HEAD_DIM, 1).astype(jnp.bfloat16)
        zero = jnp.zeros_like(kv)
        return jnp.where(left, kv, zero), jnp.where(left, zero, swapped)

    prev_lo, prev_hi = split(kv_prev)
    cur_lo, cur_hi = split(kv_cur)
    keys = jnp.concatenate([prev_lo, cur_lo, prev_hi, cur_hi], axis=0)
    key_idx = lax.broadcasted_iota(jnp.int32, (WINDOW, WINDOW), 0)
    query_idx = lax.broadcasted_iota(jnp.int32, (WINDOW, WINDOW), 1)
    from_prev = key_idx > query_idx
    weights, logs = [], []
    for pair in range(2):
        both = dot(keys, q[:, pair * LANES : (pair + 1) * LANES], ((1,), (1,)))
        for side in range(2):
            head = pair * 2 + side
            prev = both[side * 256 : side * 256 + WINDOW]
            cur = both[side * 256 + WINDOW : side * 256 + 2 * WINDOW]
            if has_prev is not None:
                prev = jnp.where(has_prev, prev, -jnp.inf)
            scores = jnp.where(from_prev, prev, cur) * HEAD_DIM ** (-0.5)
            top = jnp.maximum(jnp.max(scores, axis=0, keepdims=True), sinks[head])
            raised = jnp.exp(scores - top)
            total = jnp.sum(raised, axis=0, keepdims=True) + jnp.exp(sinks[head] - top)
            logs.append(top + jnp.log(total))
            share = raised / total
            zero = jnp.zeros_like(share)
            weights.append(
                jnp.concatenate(
                    [jnp.where(from_prev, share, zero), jnp.where(from_prev, zero, share)], axis=0
                ).astype(jnp.bfloat16)
            )
    values = jnp.concatenate([kv_prev, kv_cur], axis=0)
    outs = []
    for pair in range(2):
        got = dot(values, jnp.concatenate(weights[pair * 2 : pair * 2 + 2], axis=1), ((0,), (0,)))
        stacked = jnp.concatenate([got[HEAD_DIM:, :WINDOW], got[HEAD_DIM:, WINDOW:]], axis=0)
        outs.append(stacked.T)
    return jnp.concatenate(outs, axis=1), jnp.concatenate(logs, axis=0)


def tail_kernel(x_ref, w0, w1, w2, w3, rim_ref, out_ref):
    acc = dot(x_ref[0], w0[...])
    for c, w in ((1, w1), (2, w2), (3, w3)):
        acc = acc + dot(x_ref[c], w[...])
    out_ref[:WINDOW, :] = acc.astype(jnp.bfloat16)
    for k in range(rim_ref.shape[1] // LANES):
        out_ref[WINDOW + k * RIM : WINDOW + (k + 1) * RIM, :] = rim_ref[
            :, k * LANES : (k + 1) * LANES
        ]


def tail_rows(x, parts, rim):
    n, depth = x.shape[1], x.shape[2]
    last = n // WINDOW - 1
    rows = WINDOW + rim.shape[1] // LANES * RIM
    return pl.pallas_call(
        tail_kernel,
        grid=(1,),
        in_specs=[pl.BlockSpec((4, WINDOW, depth), lambda i: (0, last, 0))]
        + [pl.BlockSpec((depth, LANES), lambda i: (0, 0))] * 4
        + [pl.BlockSpec(rim.shape, lambda i: (0, 0))],
        out_specs=pl.BlockSpec((rows, LANES), lambda i: (0, 0)),
        out_shape=jax.ShapeDtypeStruct((rows, LANES), jnp.bfloat16),
        compiler_params=settings(6),
        cost_estimate=cost(1),
        name="tail",
    )(x, *parts, rim)


def attn_kernel(sinks, x_ref, w0, w1, w2, w3, att_ref, log_ref, rows_ref):
    n = x_ref.shape[1]
    step = 256
    parts = (w0, w1, w2, w3)
    for at in range(0, n, step):
        acc = dot(x_ref[0, at : at + step, :], w0[...])
        for c in range(1, 4):
            acc = acc + dot(x_ref[c, at : at + step, :], parts[c][...])
        rows_ref[at : at + step, :] = acc.astype(jnp.bfloat16)
    heads = [sinks[h] for h in range(4)]
    att_ref[:WINDOW, :] = jnp.zeros((WINDOW, 2 * LANES), jnp.float32)
    log_ref[:, :WINDOW] = jnp.zeros((4, WINDOW), jnp.float32)

    for b in range(1, n // WINDOW):
        here, before = b * WINDOW, (b - 1) * WINDOW
        att, logs = attend_block(
            rows_ref[here : here + WINDOW, LANES:],
            rows_ref[before : before + WINDOW, :LANES],
            rows_ref[here : here + WINDOW, :LANES],
            heads,
            None,
        )
        att_ref[here : here + WINDOW, :] = att
        log_ref[:, here : here + WINDOW] = logs


def attention(sinks, x, parts):
    n = x.shape[1]
    cols = parts[0].shape[1]
    return pl.pallas_call(
        attn_kernel,
        in_specs=[SMEM] + [VMEM] * 5,
        out_specs=[VMEM] * 3,
        out_shape=[
            jax.ShapeDtypeStruct((n, 2 * LANES), jnp.float32),
            jax.ShapeDtypeStruct((4, n), jnp.float32),
            jax.ShapeDtypeStruct((n, cols), jnp.bfloat16),
        ],
        compiler_params=settings(20),
        cost_estimate=cost(8),
        name="attn",
    )(sinks, x, *parts)


def conv_kernel(
    sinks, place, x_ref, w0, w1, w2, w3, gain_ref, taps_ref, att_ref, log_ref, rows_ref, halo_ref,
    out_ref, log_out, pad_ref, prev_x,
):
    n = x_ref.shape[1]
    width = 2 * LANES
    step = 256
    parts = (w0, w1, w2, w3)
    rim = [
        halo_ref[WINDOW + k * RIM : WINDOW + (k + 1) * RIM, :]
        for k in range(gain_ref.shape[1] // LANES)
    ]
    norm_into(place, jnp.concatenate(rim, axis=1), gain_ref[...], column_sort(), prev_x)
    acc = dot(prev_x[0], w0[:, :width])
    for c in range(1, 4):
        acc = acc + dot(prev_x[c], parts[c][:, :width])
    pad_ref[:8, :] = acc[8:16].astype(jnp.bfloat16).astype(jnp.float32)
    att0, log0 = attend_block(
        rows_ref[:WINDOW, LANES:],
        halo_ref[:WINDOW, :],
        rows_ref[:WINDOW, :LANES],
        [sinks[h] for h in range(4)],
        place[2] > 0,
    )
    log_out[...] = log_ref[...]
    log_out[:, :WINDOW] = log0
    taps = taps_ref[...].astype(jnp.float32)
    for at in range(0, n, step):
        acc = dot(x_ref[0, at : at + step, :], w0[...])
        for c in range(1, 4):
            acc = acc + dot(x_ref[c, at : at + step, :], parts[c][...])
        rounded = acc.astype(jnp.bfloat16).astype(jnp.float32)
        pad_ref[8 + at : 8 + at + step, :] = rounded[:, :width]
        total = taps[0:1] * pad_ref[6 + at : 6 + at + step, :]
        total = total + taps[1:2] * pad_ref[7 + at : 7 + at + step, :]
        total = total + taps[2:3] * rounded[:, :width]
        gated = rounded[:, width:] * total
        if at == 0:
            first = jnp.concatenate([att0, att_ref[WINDOW:step, :]], axis=0)
        else:
            first = att_ref[at : at + step, :]
        out_ref[at : at + step, :] = (first + gated).astype(jnp.bfloat16)


def convolution(sinks, place, x, parts, gain, taps, att, logs, rows, halo):
    n = x.shape[1]
    return pl.pallas_call(
        conv_kernel,
        in_specs=[SMEM] * 2 + [VMEM] * 11,
        out_specs=[VMEM] * 2,
        out_shape=[
            jax.ShapeDtypeStruct((n, 2 * LANES), jnp.bfloat16),
            jax.ShapeDtypeStruct((4, n), jnp.float32),
        ],
        scratch_shapes=[
            pltpu.VMEM((n + 8, 2 * LANES), jnp.float32),
            pltpu.VMEM((4, RIM, x.shape[2]), jnp.bfloat16),
        ],
        compiler_params=settings(20),
        cost_estimate=cost(6),
        name="conv",
    )(sinks, place, x, *parts, gain, taps, att, logs, rows, halo)


def body(
    tokens, norm_gain, w_query, w_key, w_value, w_conv_in, w_conv_gate, conv_taps, sink_logits
):
    return layer(
        tokens, norm_gain, (w_key, w_value, w_query), (w_conv_in, w_conv_gate), conv_taps, sink_logits
    )


def layer(tokens, norm_gain, attn_weights, conv_weights, conv_taps, sink_logits):
    n, width = tokens.shape
    gain = norm_gain.reshape(1, width)
    place = jnp.stack(
        [lax.axis_index("zl"), lax.axis_index("yl"), jnp.minimum(lax.axis_index(SP), 1)]
    ).astype(jnp.int32)

    mine = jnp.concatenate(attn_weights + conv_weights, axis=1)
    cut = sum(w.shape[1] for w in attn_weights)
    sent = jnp.broadcast_to(mine[None], (16,) + mine.shape)
    own = lax.all_to_all(sent, ("zh", "yh"), 0, 0)
    own = own.reshape(16 * mine.shape[0], mine.shape[1])

    def classes(block):
        corner = shift(block, -1, -1)
        along_y = shift(block, 0, 1)
        along_z = shift(block, 1, 0)
        return [block, along_y, along_z, corner]

    parts_a = classes(own[:, :cut])
    parts_b = classes(own[:, cut:])
    x = norm_classes(place, pltpu.with_memory_space_constraint(tokens, pltpu.HBM), gain, 256)
    last = tail_rows(x, parts_a, tokens[n - RIM :])
    halo = passed_along(last)
    att, logs, rows = attention(sink_logits, x, parts_a)
    return tuple(
        convolution(
            sink_logits, place, x, parts_b, gain, conv_taps, att, logs, rows, halo
        )
    )


def solution(mesh):
    fine = Mesh(
        mesh.devices.reshape(4, 2, 4, 2, mesh.shape["fs"], mesh.shape["tp"]), SP + COLS
    )
    weights = P(SP, COLS)
    return jax.shard_map(
        body,
        mesh=fine,
        in_specs=(P(SP, None), P()) + (weights,) * 5 + (P(None, COLS), P(COLS)),
        out_specs=(P(SP, COLS), P(COLS, SP)),
        check_vma=False,
    )
```

```python
import functools

import jax
import jax.numpy as jnp
from jax import lax
from jax.experimental import pallas as pl
from jax.experimental.pallas import tpu as pltpu
from jax.sharding import Mesh, PartitionSpec as P


HEAD_DIM = 64
WINDOW = 128
EPS = 1e-06

SP = ("zh", "zl", "yh", "yl")
COLS = ("fs", "tp")
SIDE = 8
LANES = 128
RIM = 16
VMEM = pl.BlockSpec(memory_space=pltpu.VMEM)
SMEM = pl.BlockSpec(memory_space=pltpu.SMEM)
HBM = pl.BlockSpec(memory_space=pltpu.HBM)


def shift(value, dz, dy):
    pairs = []
    for z in range(SIDE):
        for y in range(SIDE):
            for core, sign in enumerate((1, -1)):
                to = (z + sign * dz) % SIDE * SIDE + (y + sign * dy) % SIDE
                pairs.append(((z * SIDE + y) * 2 + core, to * 2 + core))
    return lax.ppermute(value, SP + ("tp",), pairs)


def passed_along(value):
    n = SIDE * SIDE
    return lax.ppermute(value, SP, [(i, i + 1) for i in range(n - 1)])


def settings(mib):
    return pltpu.CompilerParams(vmem_limit_bytes=mib << 20)


def cost(us):
    return pl.CostEstimate(flops=int(us * 3.9e6), bytes_accessed=1 << 20, transcendentals=0)


def dot(a, b, dims=((1,), (0,))):
    return lax.dot_general(a, b, (dims, ((), ())), preferred_element_type=jnp.float32)


def column_sort():
    span = 2 * LANES
    row = lax.broadcasted_iota(jnp.int32, (span, span), 0)
    col = lax.broadcasted_iota(jnp.int32, (span, span), 1)
    target = ((row >> 5) & 1) * LANES + (row >> 6) * 32 + (row & 31)
    return (target == col).astype(jnp.bfloat16)


def norm_into(place, rows, gain, swap, out_ref):
    widened = rows.astype(jnp.float32)
    scale = lax.rsqrt(jnp.mean(widened * widened, axis=-1, keepdims=True) + EPS)
    normed = (widened * scale * gain).astype(jnp.bfloat16)
    span = 2 * LANES
    for zh in range(4):
        for zl in range(2):
            at = (zh * 2 + zl) * span
            sorted_cols = dot(normed[:, at : at + span], swap).astype(jnp.bfloat16)
            for yl in range(2):
                into = (place[0] ^ zl) * 2 + (place[1] ^ yl)
                out_ref[into, :, zh * LANES : (zh + 1) * LANES] = sorted_cols[
                    :, yl * LANES : (yl + 1) * LANES
                ]


def norm_kernel(place, tok_hbm, gain_ref, out_hbm, *, block):
    n, width = tok_hbm.shape
    swap = column_sort()

    def step(tok_ref, out_ref):
        norm_into(place, tok_ref[...], gain_ref[...], swap, out_ref)

    pltpu.emit_pipeline(
        step,
        grid=(n // block,),
        in_specs=[pl.BlockSpec((block, width), lambda i: (i, 0))],
        out_specs=[pl.BlockSpec((4, block, width // 4), lambda i: (0, i, 0))],
    )(tok_hbm, out_hbm)


def norm_classes(place, rows, gain, block):
    n, width = rows.shape
    return pl.pallas_call(
        functools.partial(norm_kernel, block=block),
        in_specs=[SMEM, HBM, VMEM],
        out_specs=HBM,
        out_shape=pltpu.HBM((4, n, width // 4), jnp.bfloat16),
        compiler_params=settings(14),
        cost_estimate=cost(5),
        name="norm",
    )(place, rows, gain)


def attend_block(q, kv_prev, kv_cur, sinks, has_prev):
    lane = lax.broadcasted_iota(jnp.int32, (WINDOW, LANES), 1)
    left = lane < HEAD_DIM

    def split(kv):
        swapped = pltpu.roll(kv.astype(jnp.float32), HEAD_DIM, 1).astype(jnp.bfloat16)
        zero = jnp.zeros_like(kv)
        return jnp.where(left, kv, zero), jnp.where(left, zero, swapped)

    prev_lo, prev_hi = split(kv_prev)
    cur_lo, cur_hi = split(kv_cur)
    keys = jnp.concatenate([prev_lo, cur_lo, prev_hi, cur_hi], axis=0)
    key_idx = lax.broadcasted_iota(jnp.int32, (WINDOW, WINDOW), 0)
    query_idx = lax.broadcasted_iota(jnp.int32, (WINDOW, WINDOW), 1)
    from_prev = key_idx > query_idx
    weights, logs = [], []
    for pair in range(2):
        both = dot(keys, q[:, pair * LANES : (pair + 1) * LANES], ((1,), (1,)))
        for side in range(2):
            head = pair * 2 + side
            prev = both[side * 256 : side * 256 + WINDOW]
            cur = both[side * 256 + WINDOW : side * 256 + 2 * WINDOW]
            if has_prev is not None:
                prev = jnp.where(has_prev, prev, -jnp.inf)
            scores = jnp.where(from_prev, prev, cur) * HEAD_DIM ** (-0.5)
            top = jnp.maximum(jnp.max(scores, axis=0, keepdims=True), sinks[head])
            raised = jnp.exp(scores - top)
            total = jnp.sum(raised, axis=0, keepdims=True) + jnp.exp(sinks[head] - top)
            logs.append(top + jnp.log(total))
            share = raised / total
            zero = jnp.zeros_like(share)
            weights.append(
                jnp.concatenate(
                    [jnp.where(from_prev, share, zero), jnp.where(from_prev, zero, share)], axis=0
                ).astype(jnp.bfloat16)
            )
    values = jnp.concatenate([kv_prev, kv_cur], axis=0)
    outs = []
    for pair in range(2):
        got = dot(values, jnp.concatenate(weights[pair * 2 : pair * 2 + 2], axis=1), ((0,), (0,)))
        stacked = jnp.concatenate([got[HEAD_DIM:, :WINDOW], got[HEAD_DIM:, WINDOW:]], axis=0)
        outs.append(stacked.T)
    return jnp.concatenate(outs, axis=1), jnp.concatenate(logs, axis=0)


def attn_kernel(
    sinks, x_hbm, w0, w1, w2, w3, rim_ref, att_ref, log_ref, first_ref, last_ref, x_ref, rows_ref, sems
):
    n = x_ref.shape[1]
    step = 256
    parts = (w0, w1, w2, w3)
    copies = []
    for k, at in enumerate(range(0, n, step)):
        copies.append(
            pltpu.make_async_copy(
                x_hbm.at[:, at : at + step, :], x_ref.at[:, at : at + step, :], sems.at[k]
            )
        )
        copies[-1].start()
    heads = [sinks[h] for h in range(4)]
    att_ref[:WINDOW, :] = jnp.zeros((WINDOW, 2 * LANES), jnp.float32)
    log_ref[:, :WINDOW] = jnp.zeros((4, WINDOW), jnp.float32)
    for k in range(rim_ref.shape[1] // LANES):
        last_ref[WINDOW + k * RIM : WINDOW + (k + 1) * RIM, :] = rim_ref[
            :, k * LANES : (k + 1) * LANES
        ]
    for k, at in enumerate(range(0, n, step)):
        copies[k].wait()
        acc = dot(x_ref[0, at : at + step, :], w0[...])
        for c in range(1, 4):
            acc = acc + dot(x_ref[c, at : at + step, :], parts[c][...])
        rows_ref[at : at + step, :] = acc.astype(jnp.bfloat16)
        for here in range(max(at, WINDOW), at + step, WINDOW):
            before = here - WINDOW
            att, logs = attend_block(
                rows_ref[here : here + WINDOW, LANES:],
                rows_ref[before : before + WINDOW, :LANES],
                rows_ref[here : here + WINDOW, :LANES],
                heads,
                None,
            )
            att_ref[here : here + WINDOW, :] = att
            log_ref[:, here : here + WINDOW] = logs
    first_ref[...] = rows_ref[:WINDOW, :]
    last_ref[:WINDOW, :] = rows_ref[n - WINDOW : n, :LANES]


def attention(sinks, x, parts, rim):
    n = x.shape[1]
    cols = parts[0].shape[1]
    sent = WINDOW + rim.shape[1] // LANES * RIM
    return pl.pallas_call(
        attn_kernel,
        in_specs=[SMEM, HBM] + [VMEM] * 5,
        out_specs=[VMEM] * 5,
        out_shape=[
            jax.ShapeDtypeStruct((n, 2 * LANES), jnp.float32),
            jax.ShapeDtypeStruct((4, n), jnp.float32),
            jax.ShapeDtypeStruct((WINDOW, cols), jnp.bfloat16),
            jax.ShapeDtypeStruct((sent, LANES), jnp.bfloat16),
            jax.ShapeDtypeStruct(x.shape, x.dtype),
        ],
        scratch_shapes=[
            pltpu.VMEM((n, cols), jnp.bfloat16),
            pltpu.SemaphoreType.DMA((n // 256,)),
        ],
        compiler_params=settings(20),
        cost_estimate=cost(8),
        name="attn",
    )(sinks, x, *parts, rim)


def conv_kernel(
    sinks, place, x_ref, w0, w1, w2, w3, gain_ref, taps_ref, att_ref, log_ref, rows_ref, halo_ref,
    out_ref, log_out, pad_ref, prev_x,
):
    n = x_ref.shape[1]
    width = 2 * LANES
    step = 256
    parts = (w0, w1, w2, w3)
    rim = [
        halo_ref[WINDOW + k * RIM : WINDOW + (k + 1) * RIM, :]
        for k in range(gain_ref.shape[1] // LANES)
    ]
    norm_into(place, jnp.concatenate(rim, axis=1), gain_ref[...], column_sort(), prev_x)
    acc = dot(prev_x[0], w0[:, :width])
    for c in range(1, 4):
        acc = acc + dot(prev_x[c], parts[c][:, :width])
    pad_ref[:8, :] = acc[8:16].astype(jnp.bfloat16).astype(jnp.float32)
    att0, log0 = attend_block(
        rows_ref[:WINDOW, LANES:],
        halo_ref[:WINDOW, :],
        rows_ref[:WINDOW, :LANES],
        [sinks[h] for h in range(4)],
        place[2] > 0,
    )
    log_out[...] = log_ref[...]
    log_out[:, :WINDOW] = log0
    taps = taps_ref[...].astype(jnp.float32)
    for at in range(0, n, step):
        acc = dot(x_ref[0, at : at + step, :], w0[...])
        for c in range(1, 4):
            acc = acc + dot(x_ref[c, at : at + step, :], parts[c][...])
        rounded = acc.astype(jnp.bfloat16).astype(jnp.float32)
        pad_ref[8 + at : 8 + at + step, :] = rounded[:, :width]
        total = taps[0:1] * pad_ref[6 + at : 6 + at + step, :]
        total = total + taps[1:2] * pad_ref[7 + at : 7 + at + step, :]
        total = total + taps[2:3] * rounded[:, :width]
        gated = rounded[:, width:] * total
        if at == 0:
            first = jnp.concatenate([att0, att_ref[WINDOW:step, :]], axis=0)
        else:
            first = att_ref[at : at + step, :]
        out_ref[at : at + step, :] = (first + gated).astype(jnp.bfloat16)


def convolution(sinks, place, x, parts, gain, taps, att, logs, rows, halo):
    n = x.shape[1]
    return pl.pallas_call(
        conv_kernel,
        in_specs=[SMEM] * 2 + [VMEM] * 11,
        out_specs=[VMEM] * 2,
        out_shape=[
            jax.ShapeDtypeStruct((n, 2 * LANES), jnp.bfloat16),
            jax.ShapeDtypeStruct((4, n), jnp.float32),
        ],
        scratch_shapes=[
            pltpu.VMEM((n + 8, 2 * LANES), jnp.float32),
            pltpu.VMEM((4, RIM, x.shape[2]), jnp.bfloat16),
        ],
        compiler_params=settings(20),
        cost_estimate=cost(6),
        name="conv",
    )(sinks, place, x, *parts, gain, taps, att, logs, rows, halo)


def body(
    tokens, norm_gain, w_query, w_key, w_value, w_conv_in, w_conv_gate, conv_taps, sink_logits
):
    return layer(
        tokens, norm_gain, (w_key, w_value, w_query), (w_conv_in, w_conv_gate), conv_taps, sink_logits
    )


def layer(tokens, norm_gain, attn_weights, conv_weights, conv_taps, sink_logits):
    n, width = tokens.shape
    gain = norm_gain.reshape(1, width)
    place = jnp.stack(
        [lax.axis_index("zl"), lax.axis_index("yl"), jnp.minimum(lax.axis_index(SP), 1)]
    ).astype(jnp.int32)

    mine = jnp.concatenate(attn_weights + conv_weights, axis=1)
    cut = sum(w.shape[1] for w in attn_weights)
    sent = jnp.broadcast_to(mine[None], (16,) + mine.shape)
    own = lax.all_to_all(sent, ("zh", "yh"), 0, 0)
    own = own.reshape(16 * mine.shape[0], mine.shape[1])

    def classes(block):
        corner = shift(block, 1, 1)
        along_y = shift(block, 0, 1)
        along_z = shift(block, 1, 0)
        return [block, along_y, along_z, corner]

    parts_a = classes(own[:, :cut])
    parts_b = classes(own[:, cut:])
    rim = tokens[n - RIM :]
    x = norm_classes(place, pltpu.with_memory_space_constraint(tokens, pltpu.HBM), gain, 256)
    x = pltpu.with_memory_space_constraint(x, pltpu.HBM)
    att, logs, first, last, x_near = attention(sink_logits, x, parts_a, rim)
    halo = passed_along(last)
    return tuple(
        convolution(sink_logits, place, x_near, parts_b, gain, conv_taps, att, logs, first, halo)
    )


def solution(mesh):
    fine = Mesh(
        mesh.devices.reshape(4, 2, 4, 2, mesh.shape["fs"], mesh.shape["tp"]), SP + COLS
    )
    weights = P(SP, COLS)
    return jax.shard_map(
        body,
        mesh=fine,
        in_specs=(P(SP, None), P()) + (weights,) * 5 + (P(None, COLS), P(COLS)),
        out_specs=(P(SP, COLS), P(COLS, SP)),
        check_vma=False,
    )
```

```python
import jax
import jax.numpy as jnp
from jax import lax
from jax.experimental import pallas as pl
from jax.experimental.pallas import tpu as pltpu
from jax.sharding import Mesh, PartitionSpec as P


HEAD_DIM = 64
WINDOW = 128
EPS = 1e-06

SP = ("zh", "zl", "yh", "yl")
COLS = ("fs", "tp")
SIDE = 8
LANES = 128
RIM = 16
VMEM = pl.BlockSpec(memory_space=pltpu.VMEM)
SMEM = pl.BlockSpec(memory_space=pltpu.SMEM)
HBM = pl.BlockSpec(memory_space=pltpu.HBM)


def shift(value, dz, dy):
    pairs = []
    for z in range(SIDE):
        for y in range(SIDE):
            pairs.append((z * SIDE + y, (z + dz) % SIDE * SIDE + (y + dy) % SIDE))
    return lax.ppermute(value, SP, pairs)


def passed_along(value):
    n = SIDE * SIDE
    return lax.ppermute(value, SP, [(i, i + 1) for i in range(n - 1)])


def settings(mib):
    return pltpu.CompilerParams(vmem_limit_bytes=mib << 20)


def cost(us):
    return pl.CostEstimate(flops=int(us * 3.9e6), bytes_accessed=1 << 20, transcendentals=0)


def dot(a, b, dims=((1,), (0,))):
    return lax.dot_general(a, b, (dims, ((), ())), preferred_element_type=jnp.float32)


def column_sort():
    span = 2 * LANES
    row = lax.broadcasted_iota(jnp.int32, (span, span), 0)
    col = lax.broadcasted_iota(jnp.int32, (span, span), 1)
    target = ((row >> 5) & 1) * LANES + (row >> 6) * 32 + (row & 31)
    return (target == col).astype(jnp.bfloat16)


def norm_into(place, rows, gain, swap, out_ref):
    widened = rows.astype(jnp.float32)
    scale = lax.rsqrt(jnp.mean(widened * widened, axis=-1, keepdims=True) + EPS)
    normed = (widened * scale * gain).astype(jnp.bfloat16)
    span = 2 * LANES
    for zh in range(4):
        for zl in range(2):
            at = (zh * 2 + zl) * span
            sorted_cols = dot(normed[:, at : at + span], swap).astype(jnp.bfloat16)
            for yl in range(2):
                into = (place[0] ^ zl) * 2 + (place[1] ^ yl)
                out_ref[into, :, zh * LANES : (zh + 1) * LANES] = sorted_cols[
                    :, yl * LANES : (yl + 1) * LANES
                ]


def norm_kernel(place, tok_ref, gain_ref, out_ref, rim_ref):
    rim_ref[...] = tok_ref[tok_ref.shape[0] - RIM :, :]
    norm_into(place, tok_ref[...], gain_ref[...], column_sort(), out_ref)


def norm_classes(place, rows, gain, block):
    n, width = rows.shape
    return pl.pallas_call(
        norm_kernel,
        grid_spec=pltpu.PrefetchScalarGridSpec(
            num_scalar_prefetch=1,
            grid=(n // block,),
            in_specs=[
                pl.BlockSpec((block, width), lambda i, p: (i, 0)),
                pl.BlockSpec((1, width), lambda i, p: (0, 0)),
            ],
            out_specs=[
                pl.BlockSpec((4, block, width // 4), lambda i, p: (0, i, 0)),
                pl.BlockSpec((RIM, width), lambda i, p: (0, 0)),
            ],
        ),
        out_shape=[
            jax.ShapeDtypeStruct((4, n, width // 4), jnp.bfloat16),
            jax.ShapeDtypeStruct((RIM, width), jnp.bfloat16),
        ],
        compiler_params=settings(14),
        cost_estimate=cost(5),
        name="norm",
    )(place, rows, gain)


def attend_block(q, kv_prev, kv_cur, sinks, has_prev):
    lane = lax.broadcasted_iota(jnp.int32, (WINDOW, LANES), 1)
    left = lane < HEAD_DIM

    def split(kv):
        swapped = pltpu.roll(kv.astype(jnp.float32), HEAD_DIM, 1).astype(jnp.bfloat16)
        zero = jnp.zeros_like(kv)
        return jnp.where(left, kv, zero), jnp.where(left, zero, swapped)

    prev_lo, prev_hi = split(kv_prev)
    cur_lo, cur_hi = split(kv_cur)
    keys = jnp.concatenate([prev_lo, cur_lo, prev_hi, cur_hi], axis=0)
    key_idx = lax.broadcasted_iota(jnp.int32, (WINDOW, WINDOW), 0)
    query_idx = lax.broadcasted_iota(jnp.int32, (WINDOW, WINDOW), 1)
    from_prev = key_idx > query_idx
    weights, logs = [], []
    for pair in range(2):
        both = dot(keys, q[:, pair * LANES : (pair + 1) * LANES], ((1,), (1,)))
        for side in range(2):
            head = pair * 2 + side
            prev = both[side * 256 : side * 256 + WINDOW]
            cur = both[side * 256 + WINDOW : side * 256 + 2 * WINDOW]
            if has_prev is not None:
                prev = jnp.where(has_prev, prev, -jnp.inf)
            scores = jnp.where(from_prev, prev, cur) * HEAD_DIM ** (-0.5)
            top = jnp.maximum(jnp.max(scores, axis=0, keepdims=True), sinks[head])
            raised = jnp.exp(scores - top)
            total = jnp.sum(raised, axis=0, keepdims=True) + jnp.exp(sinks[head] - top)
            logs.append(top + jnp.log(total))
            share = raised / total
            zero = jnp.zeros_like(share)
            weights.append(
                jnp.concatenate(
                    [jnp.where(from_prev, share, zero), jnp.where(from_prev, zero, share)], axis=0
                ).astype(jnp.bfloat16)
            )
    values = jnp.concatenate([kv_prev, kv_cur], axis=0)
    outs = []
    for pair in range(2):
        got = dot(values, jnp.concatenate(weights[pair * 2 : pair * 2 + 2], axis=1), ((0,), (0,)))
        stacked = jnp.concatenate([got[HEAD_DIM:, :WINDOW], got[HEAD_DIM:, WINDOW:]], axis=0)
        outs.append(stacked.T)
    return jnp.concatenate(outs, axis=1), jnp.concatenate(logs, axis=0)


def tail_kernel(x_ref, w0, w1, w2, w3, rim_ref, out_ref):
    acc = dot(x_ref[0], w0[...])
    for c, w in ((1, w1), (2, w2), (3, w3)):
        acc = acc + dot(x_ref[c], w[...])
    out_ref[:WINDOW, :] = acc.astype(jnp.bfloat16)
    for k in range(rim_ref.shape[1] // LANES):
        out_ref[WINDOW + k * RIM : WINDOW + (k + 1) * RIM, :] = rim_ref[
            :, k * LANES : (k + 1) * LANES
        ]


def tail_rows(x, parts, rim):
    n, depth = x.shape[1], x.shape[2]
    last = n // WINDOW - 1
    rows = WINDOW + rim.shape[1] // LANES * RIM
    return pl.pallas_call(
        tail_kernel,
        grid=(1,),
        in_specs=[pl.BlockSpec((4, WINDOW, depth), lambda i: (0, last, 0))]
        + [pl.BlockSpec((depth, LANES), lambda i: (0, 0))] * 4
        + [pl.BlockSpec(rim.shape, lambda i: (0, 0))],
        out_specs=pl.BlockSpec((rows, LANES), lambda i: (0, 0)),
        out_shape=jax.ShapeDtypeStruct((rows, LANES), jnp.bfloat16),
        compiler_params=settings(6),
        cost_estimate=cost(1),
        name="tail",
    )(x, *parts, rim)


def attn_kernel(sinks, x_ref, w0, w1, w2, w3, att_ref, log_ref, rows_ref):
    n = x_ref.shape[1]
    step = 256
    cols = rows_ref.shape[1]
    parts = (w0, w1, w2, w3)
    for at in range(0, n, step):
        acc = dot(x_ref[0, at : at + step, :], w0[:, :cols])
        for c in range(1, 4):
            acc = acc + dot(x_ref[c, at : at + step, :], parts[c][:, :cols])
        rows_ref[at : at + step, :] = acc.astype(jnp.bfloat16)
    heads = [sinks[h] for h in range(4)]
    att_ref[:WINDOW, :] = jnp.zeros((WINDOW, 2 * LANES), jnp.float32)
    log_ref[:, :WINDOW] = jnp.zeros((4, WINDOW), jnp.float32)

    for b in range(1, n // WINDOW):
        here, before = b * WINDOW, (b - 1) * WINDOW
        att, logs = attend_block(
            rows_ref[here : here + WINDOW, LANES:],
            rows_ref[before : before + WINDOW, :LANES],
            rows_ref[here : here + WINDOW, :LANES],
            heads,
            None,
        )
        att_ref[here : here + WINDOW, :] = att
        log_ref[:, here : here + WINDOW] = logs


def attention(sinks, x, parts):
    n = x.shape[1]
    cols = parts[1].shape[1]
    return pl.pallas_call(
        attn_kernel,
        in_specs=[SMEM] + [VMEM] * 5,
        out_specs=[VMEM] * 3,
        out_shape=[
            jax.ShapeDtypeStruct((n, 2 * LANES), jnp.float32),
            jax.ShapeDtypeStruct((4, n), jnp.float32),
            jax.ShapeDtypeStruct((n, cols), jnp.bfloat16),
        ],
        compiler_params=settings(20),
        cost_estimate=cost(8),
        name="attn",
    )(sinks, x, *parts)


def conv_kernel(
    sinks, place, x_ref, w0, w1, w2, w3, gain_ref, taps_ref, att_ref, log_ref, rows_ref, halo_ref,
    out_ref, log_out, pad_ref, prev_x,
):
    n = x_ref.shape[1]
    width = 2 * LANES
    step = 256
    parts = [w[:, w.shape[1] - 2 * width :] for w in (w0, w1, w2, w3)]
    rim = [
        halo_ref[WINDOW + k * RIM : WINDOW + (k + 1) * RIM, :]
        for k in range(gain_ref.shape[1] // LANES)
    ]
    norm_into(place, jnp.concatenate(rim, axis=1), gain_ref[...], column_sort(), prev_x)
    acc = dot(prev_x[0], parts[0][:, :width])
    for c in range(1, 4):
        acc = acc + dot(prev_x[c], parts[c][:, :width])
    pad_ref[:8, :] = acc[8:16].astype(jnp.bfloat16).astype(jnp.float32)
    att0, log0 = attend_block(
        rows_ref[:WINDOW, LANES:],
        halo_ref[:WINDOW, :],
        rows_ref[:WINDOW, :LANES],
        [sinks[h] for h in range(4)],
        place[2] > 0,
    )
    log_out[...] = log_ref[...]
    log_out[:, :WINDOW] = log0
    taps = taps_ref[...].astype(jnp.float32)
    for at in range(0, n, step):
        acc = dot(x_ref[0, at : at + step, :], parts[0])
        for c in range(1, 4):
            acc = acc + dot(x_ref[c, at : at + step, :], parts[c])
        rounded = acc.astype(jnp.bfloat16).astype(jnp.float32)
        pad_ref[8 + at : 8 + at + step, :] = rounded[:, :width]
        total = taps[0:1] * pad_ref[6 + at : 6 + at + step, :]
        total = total + taps[1:2] * pad_ref[7 + at : 7 + at + step, :]
        total = total + taps[2:3] * rounded[:, :width]
        gated = rounded[:, width:] * total
        if at == 0:
            first = jnp.concatenate([att0, att_ref[WINDOW:step, :]], axis=0)
        else:
            first = att_ref[at : at + step, :]
        out_ref[at : at + step, :] = (first + gated).astype(jnp.bfloat16)


def convolution(sinks, place, x, parts, gain, taps, att, logs, rows, halo):
    n = x.shape[1]
    return pl.pallas_call(
        conv_kernel,
        in_specs=[SMEM] * 2 + [VMEM] * 11,
        out_specs=[VMEM] * 2,
        out_shape=[
            jax.ShapeDtypeStruct((n, 2 * LANES), jnp.bfloat16),
            jax.ShapeDtypeStruct((4, n), jnp.float32),
        ],
        scratch_shapes=[
            pltpu.VMEM((n + 8, 2 * LANES), jnp.float32),
            pltpu.VMEM((4, RIM, x.shape[2]), jnp.bfloat16),
        ],
        compiler_params=settings(20),
        cost_estimate=cost(6),
        name="conv",
    )(sinks, place, x, *parts, gain, taps, att, logs, rows, halo)


def body(
    tokens, norm_gain, w_query, w_key, w_value, w_conv_in, w_conv_gate, conv_taps, sink_logits
):
    return layer(
        tokens, norm_gain, (w_key, w_value, w_query), (w_conv_in, w_conv_gate), conv_taps, sink_logits
    )


def layer(tokens, norm_gain, attn_weights, conv_weights, conv_taps, sink_logits):
    _, width = tokens.shape
    gain = norm_gain.reshape(1, width)
    place = jnp.stack(
        [lax.axis_index("zl"), lax.axis_index("yl"), jnp.minimum(lax.axis_index(SP), 1)]
    ).astype(jnp.int32)

    mine = jnp.concatenate(attn_weights + conv_weights, axis=1)
    cut = sum(w.shape[1] for w in attn_weights)
    sent = jnp.broadcast_to(mine[None], (16,) + mine.shape)
    own = lax.all_to_all(sent, ("zh", "yh"), 0, 0)
    own = own.reshape(16 * mine.shape[0], mine.shape[1])

    corner = shift(own, -1, -1)

    def classes(block):
        along_y = shift(block, 0, 1)
        along_z = shift(block, 1, 0)
        return [own, along_y, along_z, corner]

    parts_a = classes(own[:, :cut])
    parts_b = classes(own[:, cut:])
    x, rim = norm_classes(place, pltpu.with_memory_space_constraint(tokens, pltpu.HBM), gain, 256)
    last = tail_rows(x, parts_a, rim)
    halo = passed_along(last)
    att, logs, rows = attention(sink_logits, x, parts_a)
    return tuple(
        convolution(
            sink_logits, place, x, parts_b, gain, conv_taps, att, logs, rows, halo
        )
    )


def solution(mesh):
    fine = Mesh(
        mesh.devices.reshape(4, 2, 4, 2, mesh.shape["fs"], mesh.shape["tp"]), SP + COLS
    )
    weights = P(SP, COLS)
    return jax.shard_map(
        body,
        mesh=fine,
        in_specs=(P(SP, None), P()) + (weights,) * 5 + (P(None, COLS), P(COLS)),
        out_specs=(P(SP, COLS), P(COLS, SP)),
        check_vma=False,
    )
```

```python
import jax
import jax.numpy as jnp
from jax import lax
from jax.experimental import pallas as pl
from jax.experimental.pallas import tpu as pltpu
from jax.sharding import Mesh, PartitionSpec as P


HEAD_DIM = 64
WINDOW = 128
EPS = 1e-06

SP = ("zh", "zl", "yh", "yl")
COLS = ("fs", "tp")
SIDE = 8
LANES = 128
RIM = 16
VMEM = pl.BlockSpec(memory_space=pltpu.VMEM)
SMEM = pl.BlockSpec(memory_space=pltpu.SMEM)
HBM = pl.BlockSpec(memory_space=pltpu.HBM)


def shift(value, dz, dy):
    pairs = []
    for z in range(SIDE):
        for y in range(SIDE):
            pairs.append((z * SIDE + y, (z + dz) % SIDE * SIDE + (y + dy) % SIDE))
    return lax.ppermute(value, SP, pairs)


def passed_along(value):
    n = SIDE * SIDE
    return lax.ppermute(value, SP, [(i, i + 1) for i in range(n - 1)])


def settings(mib):
    return pltpu.CompilerParams(vmem_limit_bytes=mib << 20)


def cost(us):
    return pl.CostEstimate(flops=int(us * 3.9e6), bytes_accessed=1 << 20, transcendentals=0)


def dot(a, b, dims=((1,), (0,))):
    return lax.dot_general(a, b, (dims, ((), ())), preferred_element_type=jnp.float32)


def column_sort():
    span = 2 * LANES
    row = lax.broadcasted_iota(jnp.int32, (span, span), 0)
    col = lax.broadcasted_iota(jnp.int32, (span, span), 1)
    target = ((row >> 5) & 1) * LANES + (row >> 6) * 32 + (row & 31)
    return (target == col).astype(jnp.bfloat16)


def norm_into(place, rows, gain, swap, out_ref):
    widened = rows.astype(jnp.float32)
    scale = lax.rsqrt(jnp.mean(widened * widened, axis=-1, keepdims=True) + EPS)
    normed = (widened * scale * gain).astype(jnp.bfloat16)
    span = 2 * LANES
    for zh in range(4):
        for zl in range(2):
            at = (zh * 2 + zl) * span
            sorted_cols = dot(normed[:, at : at + span], swap).astype(jnp.bfloat16)
            for yl in range(2):
                into = (place[0] ^ zl) * 2 + (place[1] ^ yl)
                out_ref[into, :, zh * LANES : (zh + 1) * LANES] = sorted_cols[
                    :, yl * LANES : (yl + 1) * LANES
                ]


def norm_kernel(place, tok_ref, gain_ref, out_ref, rim_ref):
    rim_ref[...] = tok_ref[tok_ref.shape[0] - RIM :, :]
    norm_into(place, tok_ref[...], gain_ref[...], column_sort(), out_ref)


def norm_classes(place, rows, gain, block):
    n, width = rows.shape
    return pl.pallas_call(
        norm_kernel,
        grid_spec=pltpu.PrefetchScalarGridSpec(
            num_scalar_prefetch=1,
            grid=(n // block,),
            in_specs=[
                pl.BlockSpec((block, width), lambda i, p: (i, 0)),
                pl.BlockSpec((1, width), lambda i, p: (0, 0)),
            ],
            out_specs=[
                pl.BlockSpec((4, block, width // 4), lambda i, p: (0, i, 0)),
                pl.BlockSpec((RIM, width), lambda i, p: (0, 0)),
            ],
        ),
        out_shape=[
            jax.ShapeDtypeStruct((4, n, width // 4), jnp.bfloat16),
            jax.ShapeDtypeStruct((RIM, width), jnp.bfloat16),
        ],
        compiler_params=settings(9),
        cost_estimate=cost(5),
        name="norm",
    )(place, rows, gain)


def attend_block(q, kv_prev, kv_cur, sinks, has_prev):
    lane = lax.broadcasted_iota(jnp.int32, (WINDOW, LANES), 1)
    left = lane < HEAD_DIM

    def split(kv):
        swapped = pltpu.roll(kv.astype(jnp.float32), HEAD_DIM, 1).astype(jnp.bfloat16)
        zero = jnp.zeros_like(kv)
        return jnp.where(left, kv, zero), jnp.where(left, zero, swapped)

    q = q * jnp.asarray(HEAD_DIM ** (-0.5), q.dtype)
    prev_lo, prev_hi = split(kv_prev)
    cur_lo, cur_hi = split(kv_cur)
    keys = jnp.concatenate([prev_lo, cur_lo, prev_hi, cur_hi], axis=0)
    key_idx = lax.broadcasted_iota(jnp.int32, (WINDOW, WINDOW), 0)
    query_idx = lax.broadcasted_iota(jnp.int32, (WINDOW, WINDOW), 1)
    from_prev = key_idx > query_idx
    weights, logs = [], []
    for pair in range(2):
        both = dot(keys, q[:, pair * LANES : (pair + 1) * LANES], ((1,), (1,)))
        for side in range(2):
            head = pair * 2 + side
            prev = both[side * 256 : side * 256 + WINDOW]
            cur = both[side * 256 + WINDOW : side * 256 + 2 * WINDOW]
            if has_prev is not None:
                prev = jnp.where(has_prev, prev, -jnp.inf)
            scores = jnp.where(from_prev, prev, cur)
            top = jnp.maximum(jnp.max(scores, axis=0, keepdims=True), sinks[head])
            raised = jnp.exp(scores - top)
            total = jnp.sum(raised, axis=0, keepdims=True) + jnp.exp(sinks[head] - top)
            logs.append(top + jnp.log(total))
            share = raised * (1.0 / total)
            zero = jnp.zeros_like(share)
            weights.append(
                jnp.concatenate(
                    [jnp.where(from_prev, share, zero), jnp.where(from_prev, zero, share)], axis=0
                ).astype(jnp.bfloat16)
            )
    values = jnp.concatenate([kv_prev, kv_cur], axis=0)
    outs = []
    for pair in range(2):
        got = dot(values, jnp.concatenate(weights[pair * 2 : pair * 2 + 2], axis=1), ((0,), (0,)))
        stacked = jnp.concatenate([got[HEAD_DIM:, :WINDOW], got[HEAD_DIM:, WINDOW:]], axis=0)
        outs.append(stacked.T)
    return jnp.concatenate(outs, axis=1), jnp.concatenate(logs, axis=0)


def cut_kernel(own_ref, a_ref, b_ref):
    cols = a_ref.shape[1]
    a_ref[...] = own_ref[:, :cols]
    b_ref[...] = own_ref[:, cols:]


def cut_columns(own, cols):
    n, width = own.shape
    return pl.pallas_call(
        cut_kernel,
        in_specs=[VMEM],
        out_specs=[VMEM] * 2,
        out_shape=[
            jax.ShapeDtypeStruct((n, cols), own.dtype),
            jax.ShapeDtypeStruct((n, width - cols), own.dtype),
        ],
        compiler_params=settings(2),
        cost_estimate=cost(1),
        name="cut",
    )(own)


def early_kernel(x_ref, own_ref, y_ref, sum_a, sum_b):
    n = x_ref.shape[1]
    cols = sum_a.shape[1]
    step = 256
    for at in range(0, n, step):
        mine = x_ref[0, at : at + step, :]
        sum_b[at : at + step, :] = dot(mine, own_ref[:, cols:])
        sum_a[at : at + step, :] = dot(mine, own_ref[:, :cols]) + dot(
            x_ref[1, at : at + step, :], y_ref[...]
        )


def early_sums(x, own, along_y):
    n = x.shape[1]
    cols = along_y.shape[1]
    return pl.pallas_call(
        early_kernel,
        in_specs=[VMEM] * 3,
        out_specs=[VMEM] * 2,
        out_shape=[
            jax.ShapeDtypeStruct((n, cols), jnp.float32),
            jax.ShapeDtypeStruct((n, own.shape[1] - cols), jnp.float32),
        ],
        compiler_params=settings(4),
        cost_estimate=cost(2),
        name="early",
    )(x, own, along_y)


def tail_kernel(x_ref, sum_ref, w2, w3, rim_ref, out_ref):
    acc = sum_ref[...] + dot(x_ref[2], w2[...]) + dot(x_ref[3], w3[...])
    out_ref[:WINDOW, :] = acc.astype(jnp.bfloat16)
    for k in range(rim_ref.shape[1] // LANES):
        out_ref[WINDOW + k * RIM : WINDOW + (k + 1) * RIM, :] = rim_ref[
            :, k * LANES : (k + 1) * LANES
        ]


def tail_rows(x, sums, parts, rim):
    n, depth = x.shape[1], x.shape[2]
    last = n // WINDOW - 1
    rows = WINDOW + rim.shape[1] // LANES * RIM
    return pl.pallas_call(
        tail_kernel,
        grid=(1,),
        in_specs=[
            pl.BlockSpec((4, WINDOW, depth), lambda i: (0, last, 0)),
            pl.BlockSpec((WINDOW, LANES), lambda i: (last, 0)),
        ]
        + [pl.BlockSpec((depth, LANES), lambda i: (0, 0))] * 2
        + [pl.BlockSpec(rim.shape, lambda i: (0, 0))],
        out_specs=pl.BlockSpec((rows, LANES), lambda i: (0, 0)),
        out_shape=jax.ShapeDtypeStruct((rows, LANES), jnp.bfloat16),
        compiler_params=settings(3),
        cost_estimate=cost(1),
        name="tail",
    )(x, sums, *parts, rim)


def attn_kernel(sinks, x_ref, sum_ref, w2, w3, att_ref, log_ref, rows_ref):
    n = x_ref.shape[1]
    step = 256
    cols = rows_ref.shape[1]
    for at in range(0, n, step):
        acc = sum_ref[at : at + step, :] + dot(x_ref[2, at : at + step, :], w2[...])
        acc = acc + dot(x_ref[3, at : at + step, :], w3[:, :cols])
        rows_ref[at : at + step, :] = acc.astype(jnp.bfloat16)
    heads = [sinks[h] for h in range(4)]
    att_ref[:WINDOW, :] = jnp.zeros((WINDOW, 2 * LANES), jnp.float32)
    log_ref[:, :WINDOW] = jnp.zeros((4, WINDOW), jnp.float32)

    for b in range(1, n // WINDOW):
        here, before = b * WINDOW, (b - 1) * WINDOW
        att, logs = attend_block(
            rows_ref[here : here + WINDOW, LANES:],
            rows_ref[before : before + WINDOW, :LANES],
            rows_ref[here : here + WINDOW, :LANES],
            heads,
            None,
        )
        att_ref[here : here + WINDOW, :] = att
        log_ref[:, here : here + WINDOW] = logs


def attention(sinks, x, sums, parts):
    n = x.shape[1]
    cols = sums.shape[1]
    return pl.pallas_call(
        attn_kernel,
        in_specs=[SMEM] + [VMEM] * 4,
        out_specs=[VMEM] * 3,
        out_shape=[
            jax.ShapeDtypeStruct((n, 2 * LANES), jnp.float32),
            jax.ShapeDtypeStruct((4, n), jnp.float32),
            jax.ShapeDtypeStruct((n, cols), jnp.bfloat16),
        ],
        compiler_params=settings(8),
        cost_estimate=cost(8),
        name="attn",
    )(sinks, x, sums, *parts)


def conv_kernel(
    sinks, place, x_ref, sum_ref, w0, w1, w2, w3, gain_ref, taps_ref, att_ref, log_ref, rows_ref, halo_ref,
    out_hbm, log_out, out_ref, pad_ref, prev_x, sems,
):
    n = x_ref.shape[1]
    width = 2 * LANES
    step = 256
    parts = [w[:, w.shape[1] - 2 * width :] for w in (w0, w1, w2, w3)]
    rim = [
        halo_ref[WINDOW + k * RIM : WINDOW + (k + 1) * RIM, :]
        for k in range(gain_ref.shape[1] // LANES)
    ]
    norm_into(place, jnp.concatenate(rim, axis=1), gain_ref[...], column_sort(), prev_x)
    acc = dot(prev_x[0], parts[0][:, :width])
    for c in range(1, 4):
        acc = acc + dot(prev_x[c], parts[c][:, :width])
    pad_ref[:8, :] = acc[8:16].astype(jnp.bfloat16).astype(jnp.float32)
    att0, log0 = attend_block(
        rows_ref[:WINDOW, LANES:],
        halo_ref[:WINDOW, :],
        rows_ref[:WINDOW, :LANES],
        [sinks[h] for h in range(4)],
        place[2] > 0,
    )
    log_out[...] = log_ref[...]
    log_out[:, :WINDOW] = log0
    taps = taps_ref[...].astype(jnp.float32)
    copies = []
    for k, at in enumerate(range(0, n, step)):
        acc = sum_ref[at : at + step, :] + dot(x_ref[1, at : at + step, :], parts[1])
        for c in range(2, 4):
            acc = acc + dot(x_ref[c, at : at + step, :], parts[c])
        rounded = acc.astype(jnp.bfloat16).astype(jnp.float32)
        pad_ref[8 + at : 8 + at + step, :] = rounded[:, :width]
        total = taps[0:1] * pad_ref[6 + at : 6 + at + step, :]
        total = total + taps[1:2] * pad_ref[7 + at : 7 + at + step, :]
        total = total + taps[2:3] * rounded[:, :width]
        gated = rounded[:, width:] * total
        if at == 0:
            first = jnp.concatenate([att0, att_ref[WINDOW:step, :]], axis=0)
        else:
            first = att_ref[at : at + step, :]
        out_ref[at : at + step, :] = (first + gated).astype(jnp.bfloat16)
        copies.append(
            pltpu.make_async_copy(
                out_ref.at[at : at + step, :], out_hbm.at[at : at + step, :], sems.at[k]
            )
        )
        copies[-1].start()
    for copy in copies:
        copy.wait()


def convolution(sinks, place, x, sums, parts, gain, taps, att, logs, rows, halo):
    n = x.shape[1]
    return pl.pallas_call(
        conv_kernel,
        in_specs=[SMEM] * 2 + [VMEM] * 12,
        out_specs=[HBM, VMEM],
        out_shape=[
            jax.ShapeDtypeStruct((n, 2 * LANES), jnp.bfloat16),
            jax.ShapeDtypeStruct((4, n), jnp.float32),
        ],
        scratch_shapes=[
            pltpu.VMEM((n, 2 * LANES), jnp.bfloat16),
            pltpu.VMEM((n + 8, 2 * LANES), jnp.float32),
            pltpu.VMEM((4, RIM, x.shape[2]), jnp.bfloat16),
            pltpu.SemaphoreType.DMA((n // 256,)),
        ],
        compiler_params=settings(8),
        cost_estimate=cost(6),
        name="conv",
    )(sinks, place, x, sums, *parts, gain, taps, att, logs, rows, halo)


def body(
    tokens, norm_gain, w_query, w_key, w_value, w_conv_in, w_conv_gate, conv_taps, sink_logits
):
    return layer(
        tokens, norm_gain, (w_key, w_value, w_query), (w_conv_in, w_conv_gate), conv_taps, sink_logits
    )


def layer(tokens, norm_gain, attn_weights, conv_weights, conv_taps, sink_logits):
    _, width = tokens.shape
    gain = norm_gain.reshape(1, width)
    place = jnp.stack(
        [lax.axis_index("zl"), lax.axis_index("yl"), jnp.minimum(lax.axis_index(SP), 1)]
    ).astype(jnp.int32)

    mine = jnp.concatenate(attn_weights + conv_weights, axis=1)
    cut = sum(w.shape[1] for w in attn_weights)
    sent = jnp.broadcast_to(mine[None], (16,) + mine.shape)
    own = lax.all_to_all(sent, ("zh", "yh"), 0, 0)
    own = own.reshape(16 * mine.shape[0], mine.shape[1])

    corner = shift(own, -1, -1)

    def classes(block):
        along_y = shift(block, 0, 1)
        along_z = shift(block, 1, 0)
        return [own, along_y, along_z, corner]

    own_a, own_b = cut_columns(own, cut)
    parts_a = classes(own_a)
    parts_b = classes(own_b)
    x, rim = norm_classes(place, pltpu.with_memory_space_constraint(tokens, pltpu.HBM), gain, 256)
    sum_a, sum_b = early_sums(x, own, parts_a[1])
    last = tail_rows(x, sum_a, parts_a[2:], rim)
    halo = passed_along(last)
    att, logs, rows = attention(sink_logits, x, sum_a, parts_a[2:])
    return tuple(
        convolution(sink_logits, place, x, sum_b, parts_b, gain, conv_taps, att, logs, rows, halo)
    )


def solution(mesh):
    fine = Mesh(
        mesh.devices.reshape(4, 2, 4, 2, mesh.shape["fs"], mesh.shape["tp"]), SP + COLS
    )
    weights = P(SP, COLS)
    return jax.shard_map(
        body,
        mesh=fine,
        in_specs=(P(SP, None), P()) + (weights,) * 5 + (P(None, COLS), P(COLS)),
        out_specs=(P(SP, COLS), P(COLS, SP)),
        check_vma=False,
    )
```

```python
import jax
import jax.numpy as jnp
from jax import lax
from jax.experimental import pallas as pl
from jax.experimental.pallas import tpu as pltpu
from jax.sharding import Mesh, PartitionSpec as P


HEAD_DIM = 64
WINDOW = 128
EPS = 1e-06

SP = ("zh", "zl", "yh", "yl")
COLS = ("fs", "tp")
SIDE = 8
LANES = 128
RIM = 16
VMEM = pl.BlockSpec(memory_space=pltpu.VMEM)
SMEM = pl.BlockSpec(memory_space=pltpu.SMEM)
HBM = pl.BlockSpec(memory_space=pltpu.HBM)


def shift(value, dz, dy):
    pairs = []
    for z in range(SIDE):
        for y in range(SIDE):
            pairs.append((z * SIDE + y, (z + dz) % SIDE * SIDE + (y + dy) % SIDE))
    return lax.ppermute(value, SP, pairs)


def passed_along(value):
    n = SIDE * SIDE
    return lax.ppermute(value, SP, [(i, i + 1) for i in range(n - 1)])


def settings(mib):
    return pltpu.CompilerParams(vmem_limit_bytes=mib << 20)


def cost(us):
    return pl.CostEstimate(flops=int(us * 3.9e6), bytes_accessed=1 << 20, transcendentals=0)


def dot(a, b, dims=((1,), (0,))):
    return lax.dot_general(a, b, (dims, ((), ())), preferred_element_type=jnp.float32)


def column_sort():
    span = 2 * LANES
    row = lax.broadcasted_iota(jnp.int32, (span, span), 0)
    col = lax.broadcasted_iota(jnp.int32, (span, span), 1)
    target = ((row >> 5) & 1) * LANES + (row >> 6) * 32 + (row & 31)
    return (target == col).astype(jnp.bfloat16)


def norm_into(place, rows, gain, swap, out_ref):
    widened = rows.astype(jnp.float32)
    scale = lax.rsqrt(jnp.mean(widened * widened, axis=-1, keepdims=True) + EPS)
    normed = (widened * scale * gain).astype(jnp.bfloat16)
    span = 2 * LANES
    for zh in range(4):
        for zl in range(2):
            at = (zh * 2 + zl) * span
            sorted_cols = dot(normed[:, at : at + span], swap).astype(jnp.bfloat16)
            for yl in range(2):
                into = (place[0] ^ zl) * 2 + (place[1] ^ yl)
                out_ref[into, :, zh * LANES : (zh + 1) * LANES] = sorted_cols[
                    :, yl * LANES : (yl + 1) * LANES
                ]


def norm_kernel(place, tok_ref, gain_ref, out_ref, rim_ref):
    rim_ref[...] = tok_ref[tok_ref.shape[0] - RIM :, :]
    norm_into(place, tok_ref[...], gain_ref[...], column_sort(), out_ref)


def norm_classes(place, rows, gain, block):
    n, width = rows.shape
    return pl.pallas_call(
        norm_kernel,
        grid_spec=pltpu.PrefetchScalarGridSpec(
            num_scalar_prefetch=1,
            grid=(n // block,),
            in_specs=[
                pl.BlockSpec((block, width), lambda i, p: (i, 0)),
                pl.BlockSpec((1, width), lambda i, p: (0, 0)),
            ],
            out_specs=[
                pl.BlockSpec((4, block, width // 4), lambda i, p: (0, i, 0)),
                pl.BlockSpec((RIM, width), lambda i, p: (0, 0)),
            ],
        ),
        out_shape=[
            jax.ShapeDtypeStruct((4, n, width // 4), jnp.bfloat16),
            jax.ShapeDtypeStruct((RIM, width), jnp.bfloat16),
        ],
        compiler_params=settings(9),
        cost_estimate=cost(5),
        name="norm",
    )(place, rows, gain)


def attend_block(q, kv_prev, kv_cur, sinks, has_prev):
    lane = lax.broadcasted_iota(jnp.int32, (WINDOW, LANES), 1)
    left = lane < HEAD_DIM

    def split(kv):
        swapped = pltpu.roll(kv.astype(jnp.float32), HEAD_DIM, 1).astype(jnp.bfloat16)
        zero = jnp.zeros_like(kv)
        return jnp.where(left, kv, zero), jnp.where(left, zero, swapped)

    q = q * jnp.asarray(HEAD_DIM ** (-0.5), q.dtype)
    prev_lo, prev_hi = split(kv_prev)
    cur_lo, cur_hi = split(kv_cur)
    keys = jnp.concatenate([prev_lo, cur_lo, prev_hi, cur_hi], axis=0)
    key_idx = lax.broadcasted_iota(jnp.int32, (WINDOW, WINDOW), 0)
    query_idx = lax.broadcasted_iota(jnp.int32, (WINDOW, WINDOW), 1)
    from_prev = key_idx > query_idx
    weights, logs = [], []
    for pair in range(2):
        both = dot(keys, q[:, pair * LANES : (pair + 1) * LANES], ((1,), (1,)))
        for side in range(2):
            head = pair * 2 + side
            prev = both[side * 256 : side * 256 + WINDOW]
            cur = both[side * 256 + WINDOW : side * 256 + 2 * WINDOW]
            if has_prev is not None:
                prev = jnp.where(has_prev, prev, -jnp.inf)
            scores = jnp.where(from_prev, prev, cur)
            top = jnp.maximum(jnp.max(scores, axis=0, keepdims=True), sinks[head])
            raised = jnp.exp(scores - top)
            total = jnp.sum(raised, axis=0, keepdims=True) + jnp.exp(sinks[head] - top)
            logs.append(top + jnp.log(total))
            share = raised * (1.0 / total)
            zero = jnp.zeros_like(share)
            weights.append(
                jnp.concatenate(
                    [jnp.where(from_prev, share, zero), jnp.where(from_prev, zero, share)], axis=0
                ).astype(jnp.bfloat16)
            )
    values = jnp.concatenate([kv_prev, kv_cur], axis=0)
    outs = []
    for pair in range(2):
        got = dot(values, jnp.concatenate(weights[pair * 2 : pair * 2 + 2], axis=1), ((0,), (0,)))
        stacked = jnp.concatenate([got[HEAD_DIM:, :WINDOW], got[HEAD_DIM:, WINDOW:]], axis=0)
        outs.append(stacked.T)
    return jnp.concatenate(outs, axis=1), jnp.concatenate(logs, axis=0)


def cut_kernel(own_ref, a_ref, b_ref):
    cols = a_ref.shape[1]
    a_ref[...] = own_ref[:, :cols]
    b_ref[...] = own_ref[:, cols:]


def cut_columns(own, cols):
    n, width = own.shape
    return pl.pallas_call(
        cut_kernel,
        in_specs=[VMEM],
        out_specs=[VMEM] * 2,
        out_shape=[
            jax.ShapeDtypeStruct((n, cols), own.dtype),
            jax.ShapeDtypeStruct((n, width - cols), own.dtype),
        ],
        compiler_params=settings(2),
        cost_estimate=cost(1),
        name="cut",
    )(own)


def early_kernel(x_ref, own_ref, y_ref, z_ref, sum_ref):
    n = x_ref.shape[1]
    cols = sum_ref.shape[1]
    step = 512
    for at in range(0, n, step):
        acc = dot(x_ref[0, at : at + step, :], own_ref[:, :cols])
        acc = acc + dot(x_ref[1, at : at + step, :], y_ref[...])
        sum_ref[at : at + step, :] = acc + dot(x_ref[2, at : at + step, :], z_ref[...])


def early_sums(x, own, along_y, along_z):
    n = x.shape[1]
    cols = along_y.shape[1]
    return pl.pallas_call(
        early_kernel,
        in_specs=[VMEM] * 4,
        out_specs=VMEM,
        out_shape=jax.ShapeDtypeStruct((n, cols), jnp.float32),
        compiler_params=settings(4),
        cost_estimate=cost(2),
        name="early",
    )(x, own, along_y, along_z)


def attn_kernel(
    sinks, x_ref, sum_ref, own_ref, corner_ref, rim_ref, att_ref, log_ref, first_ref, last_ref, sum_b, rows_ref
):
    n = x_ref.shape[1]
    step = 256
    cols = rows_ref.shape[1]
    heads = [sinks[h] for h in range(4)]
    log_ref[:, :WINDOW] = jnp.zeros((4, WINDOW), jnp.float32)
    for k in range(rim_ref.shape[1] // LANES):
        last_ref[WINDOW + k * RIM : WINDOW + (k + 1) * RIM, :] = rim_ref[
            :, k * LANES : (k + 1) * LANES
        ]
    for at in range(0, n, step):
        far = x_ref[3, at : at + step, :]
        acc = sum_ref[at : at + step, :] + dot(far, corner_ref[:, :cols])
        rows_ref[at : at + step, :] = acc.astype(jnp.bfloat16)
        sum_b[at : at + step, :] = dot(far, corner_ref[:, cols:]) + dot(
            x_ref[0, at : at + step, :], own_ref[:, cols:]
        )
    first_ref[...] = rows_ref[:WINDOW, :]
    last_ref[:WINDOW, :] = rows_ref[n - WINDOW : n, :LANES]
    for b in range(1, n // WINDOW):
        here, before = b * WINDOW, (b - 1) * WINDOW
        att, logs = attend_block(
            rows_ref[here : here + WINDOW, LANES:],
            rows_ref[before : before + WINDOW, :LANES],
            rows_ref[here : here + WINDOW, :LANES],
            heads,
            None,
        )
        att_ref[before : before + WINDOW, :] = att
        log_ref[:, here : here + WINDOW] = logs


def attention(sinks, x, sums, own, corner, rim):
    n = x.shape[1]
    cols = sums.shape[1]
    return pl.pallas_call(
        attn_kernel,
        in_specs=[SMEM] + [VMEM] * 5,
        out_specs=[VMEM] * 5,
        out_shape=[
            jax.ShapeDtypeStruct((n - WINDOW, 2 * LANES), jnp.float32),
            jax.ShapeDtypeStruct((4, n), jnp.float32),
            jax.ShapeDtypeStruct((WINDOW, cols), jnp.bfloat16),
            jax.ShapeDtypeStruct((WINDOW + rim.shape[1] // LANES * RIM, LANES), jnp.bfloat16),
            jax.ShapeDtypeStruct((n, own.shape[1] - cols), jnp.float32),
        ],
        scratch_shapes=[pltpu.VMEM((n, cols), jnp.bfloat16)],
        compiler_params=settings(8),
        cost_estimate=cost(6),
        name="attn",
    )(sinks, x, sums, own, corner, rim)


def conv_kernel(
    x_ref, sum_ref, y_ref, z_ref, taps_ref, att_ref, log_ref,
    out_hbm, log_hbm, first_ref, out_ref, pad_ref, sems, log_sem,
):
    n = x_ref.shape[1]
    width = 2 * LANES
    step = 256
    log_copy = pltpu.make_async_copy(log_ref, log_hbm, log_sem)
    log_copy.start()
    taps = taps_ref[...].astype(jnp.float32)
    copies = []
    for k, at in enumerate(range(0, n, step)):
        acc = sum_ref[at : at + step, :] + dot(x_ref[1, at : at + step, :], y_ref[...])
        acc = acc + dot(x_ref[2, at : at + step, :], z_ref[...])
        rounded = acc.astype(jnp.bfloat16)
        low = 0
        if at == 0:
            first_ref[...] = rounded[:WINDOW, :]
            low = WINDOW
        rounded = rounded.astype(jnp.float32)
        pad_ref[at : at + step, :] = rounded[:, :width]
        total = taps[0:1] * pad_ref[at + low - 2 : at + step - 2, :]
        total = total + taps[1:2] * pad_ref[at + low - 1 : at + step - 1, :]
        total = total + taps[2:3] * rounded[low:, :width]
        gated = rounded[low:, width:] * total
        summed = att_ref[at + low - WINDOW : at + step - WINDOW, :] + gated
        out_ref[at + low : at + step, :] = summed.astype(jnp.bfloat16)
        copies.append(
            pltpu.make_async_copy(
                out_ref.at[at + low : at + step, :], out_hbm.at[at + low : at + step, :], sems.at[k]
            )
        )
        copies[-1].start()
    for copy in copies:
        copy.wait()
    log_copy.wait()


def convolution(x, sums, along_y, along_z, taps, att, logs):
    n = x.shape[1]
    return pl.pallas_call(
        conv_kernel,
        in_specs=[VMEM] * 7,
        out_specs=[HBM, HBM, VMEM],
        out_shape=[
            jax.ShapeDtypeStruct((n, 2 * LANES), jnp.bfloat16),
            jax.ShapeDtypeStruct((4, n), jnp.float32),
            jax.ShapeDtypeStruct((WINDOW, 4 * LANES), jnp.bfloat16),
        ],
        scratch_shapes=[
            pltpu.VMEM((n, 2 * LANES), jnp.bfloat16),
            pltpu.VMEM((n, 2 * LANES), jnp.float32),
            pltpu.SemaphoreType.DMA((n // 256,)),
            pltpu.SemaphoreType.DMA(()),
        ],
        compiler_params=settings(8),
        cost_estimate=cost(4),
        name="conv",
    )(x, sums, along_y, along_z, taps, att, logs)


def head_kernel(
    sinks, place, w0, w1, w2, w3, gain_ref, taps_ref, rows_ref, conv_ref, halo_ref, out_in, log_in,
    out_hbm, log_hbm, out_ref, log_ref, pad_ref, prev_x, sem, log_sem,
):
    width = 2 * LANES
    att, logs = attend_block(
        rows_ref[:, LANES:],
        halo_ref[:WINDOW, :],
        rows_ref[:, :LANES],
        [sinks[h] for h in range(4)],
        place[2] > 0,
    )
    log_ref[...] = logs
    log_copy = pltpu.make_async_copy(log_ref, log_hbm.at[:, :WINDOW], log_sem)
    log_copy.start()
    rim = [
        halo_ref[WINDOW + k * RIM : WINDOW + (k + 1) * RIM, :]
        for k in range(gain_ref.shape[1] // LANES)
    ]
    norm_into(place, jnp.concatenate(rim, axis=1), gain_ref[...], column_sort(), prev_x)
    parts = [w[:, w.shape[1] - 2 * width : w.shape[1] - width] for w in (w0, w1, w2, w3)]
    acc = dot(prev_x[0], parts[0])
    for c in range(1, 4):
        acc = acc + dot(prev_x[c], parts[c])
    pad_ref[:8, :] = acc[8:16].astype(jnp.bfloat16).astype(jnp.float32)
    taps = taps_ref[...].astype(jnp.float32)
    rounded = conv_ref[...].astype(jnp.float32)
    pad_ref[8:, :] = rounded[:, :width]
    total = taps[0:1] * pad_ref[6 : 6 + WINDOW, :]
    total = total + taps[1:2] * pad_ref[7 : 7 + WINDOW, :]
    total = total + taps[2:3] * rounded[:, :width]
    out_ref[...] = (att + rounded[:, width:] * total).astype(jnp.bfloat16)
    copy = pltpu.make_async_copy(out_ref, out_hbm.at[:WINDOW, :], sem)
    copy.start()
    copy.wait()
    log_copy.wait()


def head(sinks, place, parts, gain, taps, rows, conv_rows, halo, mixed, logs):
    return pl.pallas_call(
        head_kernel,
        in_specs=[SMEM] * 2 + [VMEM] * 9 + [HBM] * 2,
        out_specs=[HBM, HBM],
        out_shape=[
            jax.ShapeDtypeStruct(mixed.shape, mixed.dtype),
            jax.ShapeDtypeStruct(logs.shape, logs.dtype),
        ],
        input_output_aliases={11: 0, 12: 1},
        scratch_shapes=[
            pltpu.VMEM((WINDOW, 2 * LANES), jnp.bfloat16),
            pltpu.VMEM((4, WINDOW), jnp.float32),
            pltpu.VMEM((WINDOW + 8, 2 * LANES), jnp.float32),
            pltpu.VMEM((4, RIM, parts[0].shape[0]), jnp.bfloat16),
            pltpu.SemaphoreType.DMA(()),
            pltpu.SemaphoreType.DMA(()),
        ],
        compiler_params=settings(6),
        cost_estimate=cost(2),
        name="head",
    )(sinks, place, *parts, gain, taps, rows, conv_rows, halo, mixed, logs)


def body(
    tokens, norm_gain, w_query, w_key, w_value, w_conv_in, w_conv_gate, conv_taps, sink_logits
):
    return layer(
        tokens, norm_gain, (w_key, w_value, w_query), (w_conv_in, w_conv_gate), conv_taps, sink_logits
    )


def layer(tokens, norm_gain, attn_weights, conv_weights, conv_taps, sink_logits):
    _, width = tokens.shape
    gain = norm_gain.reshape(1, width)
    place = jnp.stack(
        [lax.axis_index("zl"), lax.axis_index("yl"), jnp.minimum(lax.axis_index(SP), 1)]
    ).astype(jnp.int32)

    mine = jnp.concatenate(attn_weights + conv_weights, axis=1)
    cut = sum(w.shape[1] for w in attn_weights)
    sent = jnp.broadcast_to(mine[None], (16,) + mine.shape)
    own = lax.all_to_all(sent, ("zh", "yh"), 0, 0)
    own = own.reshape(16 * mine.shape[0], mine.shape[1])

    corner = shift(own, -1, -1)

    def classes(block):
        along_y = shift(block, 0, 1)
        along_z = shift(block, 1, 0)
        return [own, along_y, along_z, corner]

    own_a, own_b = cut_columns(own, cut)
    parts_a = classes(own_a)
    parts_b = classes(own_b)
    near = pltpu.with_memory_space_constraint
    x, rim = norm_classes(place, near(tokens, pltpu.HBM), near(gain, pltpu.HBM), 256)
    sum_a = early_sums(x, own, parts_a[1], parts_a[2])
    att, logs, rows, last, sum_b = attention(sink_logits, x, sum_a, own, corner, rim)
    halo = passed_along(last)
    mixed, logs, conv_rows = convolution(
        x, sum_b, parts_b[1], parts_b[2], conv_taps, att, logs
    )
    return tuple(
        head(
            sink_logits, place, parts_b, gain, conv_taps, rows, conv_rows, halo, mixed, logs
        )
    )


def solution(mesh):
    fine = Mesh(
        mesh.devices.reshape(4, 2, 4, 2, mesh.shape["fs"], mesh.shape["tp"]), SP + COLS
    )
    weights = P(SP, COLS)
    return jax.shard_map(
        body,
        mesh=fine,
        in_specs=(P(SP, None), P()) + (weights,) * 5 + (P(None, COLS), P(COLS)),
        out_specs=(P(SP, COLS), P(COLS, SP)),
        check_vma=False,
    )
```

```python
import jax
import jax.numpy as jnp
from jax import lax
from jax.experimental import pallas as pl
from jax.experimental.pallas import tpu as pltpu
from jax.sharding import Mesh, PartitionSpec as P


HEAD_DIM = 64
WINDOW = 128
EPS = 1e-06

SP = ("zh", "zl", "yh", "yl")
COLS = ("fs", "tp")
SIDE = 8
LANES = 128
RIM = 16
VMEM = pl.BlockSpec(memory_space=pltpu.VMEM)
SMEM = pl.BlockSpec(memory_space=pltpu.SMEM)
HBM = pl.BlockSpec(memory_space=pltpu.HBM)


def shift(value, dz, dy):
    pairs = []
    for z in range(SIDE):
        for y in range(SIDE):
            pairs.append((z * SIDE + y, (z + dz) % SIDE * SIDE + (y + dy) % SIDE))
    return lax.ppermute(value, SP, pairs)


def passed_along(value):
    n = SIDE * SIDE
    return lax.ppermute(value, SP, [(i, i + 1) for i in range(n - 1)])


def settings(mib):
    return pltpu.CompilerParams(vmem_limit_bytes=mib << 20)


def cost(us):
    return pl.CostEstimate(flops=int(us * 3.9e6), bytes_accessed=1 << 20, transcendentals=0)


def dot(a, b, dims=((1,), (0,))):
    return lax.dot_general(a, b, (dims, ((), ())), preferred_element_type=jnp.float32)


def column_sort():
    span = 2 * LANES
    row = lax.broadcasted_iota(jnp.int32, (span, span), 0)
    col = lax.broadcasted_iota(jnp.int32, (span, span), 1)
    target = ((row >> 5) & 1) * LANES + (row >> 6) * 32 + (row & 31)
    return (target == col).astype(jnp.bfloat16)


def norm_into(place, rows, gain, swap, out_ref):
    widened = rows.astype(jnp.float32)
    scale = lax.rsqrt(jnp.mean(widened * widened, axis=-1, keepdims=True) + EPS)
    normed = (widened * scale * gain).astype(jnp.bfloat16)
    span = 2 * LANES
    for zh in range(4):
        for zl in range(2):
            at = (zh * 2 + zl) * span
            sorted_cols = dot(normed[:, at : at + span], swap).astype(jnp.bfloat16)
            for yl in range(2):
                into = (place[0] ^ zl) * 2 + (place[1] ^ yl)
                out_ref[into, :, zh * LANES : (zh + 1) * LANES] = sorted_cols[
                    :, yl * LANES : (yl + 1) * LANES
                ]


def norm_kernel(place, tok_ref, gain_ref, out_ref, rim_ref):
    rim_ref[...] = tok_ref[tok_ref.shape[0] - RIM :, :]
    norm_into(place, tok_ref[...], gain_ref[...], column_sort(), out_ref)


def norm_classes(place, rows, gain, block):
    n, width = rows.shape
    return pl.pallas_call(
        norm_kernel,
        grid_spec=pltpu.PrefetchScalarGridSpec(
            num_scalar_prefetch=1,
            grid=(n // block,),
            in_specs=[
                pl.BlockSpec((block, width), lambda i, p: (i, 0)),
                pl.BlockSpec((1, width), lambda i, p: (0, 0)),
            ],
            out_specs=[
                pl.BlockSpec((4, block, width // 4), lambda i, p: (0, i, 0)),
                pl.BlockSpec((RIM, width), lambda i, p: (0, 0)),
            ],
        ),
        out_shape=[
            jax.ShapeDtypeStruct((4, n, width // 4), jnp.bfloat16),
            jax.ShapeDtypeStruct((RIM, width), jnp.bfloat16),
        ],
        compiler_params=settings(9),
        cost_estimate=cost(5),
        name="norm",
    )(place, rows, gain)


def key_copies(kv):
    left = lax.broadcasted_iota(jnp.int32, kv.shape, 1) < HEAD_DIM
    swapped = pltpu.roll(kv.astype(jnp.float32), HEAD_DIM, 1).astype(kv.dtype)
    zero = jnp.zeros_like(kv)
    return jnp.where(left, kv, zero), jnp.where(left, zero, swapped)


def attend_block(q, keys_lo, keys_hi, values, sinks, has_prev):
    q = q * jnp.asarray(HEAD_DIM ** (-0.5), q.dtype)
    keys = jnp.concatenate([keys_lo, keys_hi], axis=0)
    key_idx = lax.broadcasted_iota(jnp.int32, (WINDOW, WINDOW), 0)
    query_idx = lax.broadcasted_iota(jnp.int32, (WINDOW, WINDOW), 1)
    from_prev = key_idx > query_idx
    weights, logs = [], []
    for pair in range(2):
        both = dot(keys, q[:, pair * LANES : (pair + 1) * LANES], ((1,), (1,)))
        for side in range(2):
            head = pair * 2 + side
            prev = both[side * 256 : side * 256 + WINDOW]
            cur = both[side * 256 + WINDOW : side * 256 + 2 * WINDOW]
            if has_prev is not None:
                prev = jnp.where(has_prev, prev, -jnp.inf)
            scores = jnp.where(from_prev, prev, cur)
            top = jnp.maximum(jnp.max(scores, axis=0, keepdims=True), sinks[head])
            raised = jnp.exp(scores - top)
            total = jnp.sum(raised, axis=0, keepdims=True) + jnp.exp(sinks[head] - top)
            logs.append(top + jnp.log(total))
            share = raised * (1.0 / total)
            zero = jnp.zeros_like(share)
            weights.append(
                jnp.concatenate(
                    [jnp.where(from_prev, share, zero), jnp.where(from_prev, zero, share)], axis=0
                ).astype(jnp.bfloat16)
            )
    outs = []
    for pair in range(2):
        got = dot(values, jnp.concatenate(weights[pair * 2 : pair * 2 + 2], axis=1), ((0,), (0,)))
        stacked = jnp.concatenate([got[HEAD_DIM:, :WINDOW], got[HEAD_DIM:, WINDOW:]], axis=0)
        outs.append(stacked.T)
    return jnp.concatenate(outs, axis=1), jnp.concatenate(logs, axis=0)


def cut_kernel(own_ref, a_ref, b_ref):
    cols = a_ref.shape[1]
    a_ref[...] = own_ref[:, :cols]
    b_ref[...] = own_ref[:, cols:]


def cut_columns(own, cols):
    n, width = own.shape
    return pl.pallas_call(
        cut_kernel,
        in_specs=[VMEM],
        out_specs=[VMEM] * 2,
        out_shape=[
            jax.ShapeDtypeStruct((n, cols), own.dtype),
            jax.ShapeDtypeStruct((n, width - cols), own.dtype),
        ],
        compiler_params=settings(2),
        cost_estimate=cost(1),
        name="cut",
    )(own)


def early_kernel(x_ref, own_ref, y_ref, sum_ref):
    n = x_ref.shape[1]
    cols = sum_ref.shape[1]
    step = 256
    for at in range(0, n, step):
        sum_ref[at : at + step, :] = dot(x_ref[0, at : at + step, :], own_ref[:, :cols]) + dot(
            x_ref[1, at : at + step, :], y_ref[...]
        )


def early_sums(x, own, along_y):
    n = x.shape[1]
    cols = along_y.shape[1]
    return pl.pallas_call(
        early_kernel,
        in_specs=[VMEM] * 3,
        out_specs=VMEM,
        out_shape=jax.ShapeDtypeStruct((n, cols), jnp.float32),
        compiler_params=settings(4),
        cost_estimate=cost(2),
        name="early",
    )(x, own, along_y)


def tail_kernel(x_ref, sum_ref, w2, w3, rim_ref, out_ref):
    acc = sum_ref[...] + dot(x_ref[2], w2[...]) + dot(x_ref[3], w3[...])
    out_ref[:WINDOW, :] = acc.astype(jnp.bfloat16)
    for k in range(rim_ref.shape[1] // LANES):
        out_ref[WINDOW + k * RIM : WINDOW + (k + 1) * RIM, :] = rim_ref[
            :, k * LANES : (k + 1) * LANES
        ]


def tail_rows(x, sums, parts, rim):
    n, depth = x.shape[1], x.shape[2]
    last = n // WINDOW - 1
    rows = WINDOW + rim.shape[1] // LANES * RIM
    return pl.pallas_call(
        tail_kernel,
        grid=(1,),
        in_specs=[
            pl.BlockSpec((4, WINDOW, depth), lambda i: (0, last, 0)),
            pl.BlockSpec((WINDOW, LANES), lambda i: (last, 0)),
        ]
        + [pl.BlockSpec((depth, LANES), lambda i: (0, 0))] * 2
        + [pl.BlockSpec(rim.shape, lambda i: (0, 0))],
        out_specs=pl.BlockSpec((rows, LANES), lambda i: (0, 0)),
        out_shape=jax.ShapeDtypeStruct((rows, LANES), jnp.bfloat16),
        compiler_params=settings(3),
        cost_estimate=cost(1),
        name="tail",
    )(x, sums, *parts, rim)


def attn_kernel(sinks, x_ref, sum_ref, w2, w3, att_ref, log_ref, rows_ref, lo_ref, hi_ref):
    n = x_ref.shape[1]
    step = 256
    cols = rows_ref.shape[1]
    for at in range(0, n, step):
        acc = sum_ref[at : at + step, :] + dot(x_ref[2, at : at + step, :], w2[...])
        acc = acc + dot(x_ref[3, at : at + step, :], w3[:, :cols])
        rows = acc.astype(jnp.bfloat16)
        rows_ref[at : at + step, :] = rows
        lo_ref[at : at + step, :], hi_ref[at : at + step, :] = key_copies(rows[:, :LANES])
    heads = [sinks[h] for h in range(4)]
    att_ref[:WINDOW, :] = jnp.zeros((WINDOW, 2 * LANES), jnp.float32)
    log_ref[:, :WINDOW] = jnp.zeros((4, WINDOW), jnp.float32)

    for b in range(1, n // WINDOW):
        here, before = b * WINDOW, (b - 1) * WINDOW
        att, logs = attend_block(
            rows_ref[here : here + WINDOW, LANES:],
            lo_ref[before : here + WINDOW, :],
            hi_ref[before : here + WINDOW, :],
            rows_ref[before : here + WINDOW, :LANES],
            heads,
            None,
        )
        att_ref[here : here + WINDOW, :] = att
        log_ref[:, here : here + WINDOW] = logs


def attention(sinks, x, sums, parts):
    n = x.shape[1]
    cols = sums.shape[1]
    return pl.pallas_call(
        attn_kernel,
        in_specs=[SMEM] + [VMEM] * 4,
        out_specs=[VMEM] * 3,
        out_shape=[
            jax.ShapeDtypeStruct((n, 2 * LANES), jnp.float32),
            jax.ShapeDtypeStruct((4, n), jnp.float32),
            jax.ShapeDtypeStruct((n, cols), jnp.bfloat16),
        ],
        scratch_shapes=[pltpu.VMEM((n, LANES), jnp.bfloat16)] * 2,
        compiler_params=settings(8),
        cost_estimate=cost(8),
        name="attn",
    )(sinks, x, sums, *parts)


def conv_kernel(
    sinks, place, x_ref, w0, w1, w2, w3, gain_ref, taps_ref, att_ref, log_ref, rows_ref, halo_ref,
    out_hbm, log_out, out_ref, pad_ref, prev_x, sems,
):
    n = x_ref.shape[1]
    width = 2 * LANES
    step = 256
    parts = [w[:, w.shape[1] - 2 * width :] for w in (w0, w1, w2, w3)]
    rim = [
        halo_ref[WINDOW + k * RIM : WINDOW + (k + 1) * RIM, :]
        for k in range(gain_ref.shape[1] // LANES)
    ]
    norm_into(place, jnp.concatenate(rim, axis=1), gain_ref[...], column_sort(), prev_x)
    acc = dot(prev_x[0], parts[0][:, :width])
    for c in range(1, 4):
        acc = acc + dot(prev_x[c], parts[c][:, :width])
    pad_ref[:8, :] = acc[8:16].astype(jnp.bfloat16).astype(jnp.float32)
    span = jnp.concatenate([halo_ref[:WINDOW, :], rows_ref[:WINDOW, :LANES]], axis=0)
    att0, log0 = attend_block(
        rows_ref[:WINDOW, LANES:],
        *key_copies(span),
        span,
        [sinks[h] for h in range(4)],
        place[2] > 0,
    )
    log_out[...] = log_ref[...]
    log_out[:, :WINDOW] = log0
    taps = taps_ref[...].astype(jnp.float32)
    copies = []
    for k, at in enumerate(range(0, n, step)):
        acc = dot(x_ref[0, at : at + step, :], parts[0])
        for c in range(1, 4):
            acc = acc + dot(x_ref[c, at : at + step, :], parts[c])
        rounded = acc.astype(jnp.bfloat16).astype(jnp.float32)
        pad_ref[8 + at : 8 + at + step, :] = rounded[:, :width]
        total = taps[0:1] * pad_ref[6 + at : 6 + at + step, :]
        total = total + taps[1:2] * pad_ref[7 + at : 7 + at + step, :]
        total = total + taps[2:3] * rounded[:, :width]
        gated = rounded[:, width:] * total
        if at == 0:
            first = jnp.concatenate([att0, att_ref[WINDOW:step, :]], axis=0)
        else:
            first = att_ref[at : at + step, :]
        out_ref[at : at + step, :] = (first + gated).astype(jnp.bfloat16)
        copies.append(
            pltpu.make_async_copy(
                out_ref.at[at : at + step, :], out_hbm.at[at : at + step, :], sems.at[k]
            )
        )
        copies[-1].start()
    for copy in copies:
        copy.wait()


def convolution(sinks, place, x, parts, gain, taps, att, logs, rows, halo):
    n = x.shape[1]
    return pl.pallas_call(
        conv_kernel,
        in_specs=[SMEM] * 2 + [VMEM] * 11,
        out_specs=[HBM, VMEM],
        out_shape=[
            jax.ShapeDtypeStruct((n, 2 * LANES), jnp.bfloat16),
            jax.ShapeDtypeStruct((4, n), jnp.float32),
        ],
        scratch_shapes=[
            pltpu.VMEM((n, 2 * LANES), jnp.bfloat16),
            pltpu.VMEM((n + 8, 2 * LANES), jnp.float32),
            pltpu.VMEM((4, RIM, x.shape[2]), jnp.bfloat16),
            pltpu.SemaphoreType.DMA((n // 256,)),
        ],
        compiler_params=settings(8),
        cost_estimate=cost(6),
        name="conv",
    )(sinks, place, x, *parts, gain, taps, att, logs, rows, halo)


def body(
    tokens, norm_gain, w_query, w_key, w_value, w_conv_in, w_conv_gate, conv_taps, sink_logits
):
    return layer(
        tokens, norm_gain, (w_key, w_value, w_query), (w_conv_in, w_conv_gate), conv_taps, sink_logits
    )


def layer(tokens, norm_gain, attn_weights, conv_weights, conv_taps, sink_logits):
    _, width = tokens.shape
    gain = norm_gain.reshape(1, width)
    place = jnp.stack(
        [lax.axis_index("zl"), lax.axis_index("yl"), jnp.minimum(lax.axis_index(SP), 1)]
    ).astype(jnp.int32)

    mine = jnp.concatenate(attn_weights + conv_weights, axis=1)
    cut = sum(w.shape[1] for w in attn_weights)
    sent = jnp.broadcast_to(mine[None], (16,) + mine.shape)
    own = lax.all_to_all(sent, ("zh", "yh"), 0, 0)
    own = own.reshape(16 * mine.shape[0], mine.shape[1])

    corner = shift(own, -1, -1)

    def classes(block):
        along_y = shift(block, 0, 1)
        along_z = shift(block, 1, 0)
        return [own, along_y, along_z, corner]

    own_a, own_b = cut_columns(own, cut)
    parts_a = classes(own_a)
    parts_b = classes(own_b)
    near = pltpu.with_memory_space_constraint
    x, rim = norm_classes(place, near(tokens, pltpu.HBM), near(gain, pltpu.HBM), 256)
    sum_a = early_sums(x, own, parts_a[1])
    last = tail_rows(x, sum_a, parts_a[2:], rim)
    halo = passed_along(last)
    att, logs, rows = attention(sink_logits, x, sum_a, parts_a[2:])
    return tuple(
        convolution(
            sink_logits, place, x, parts_b, gain, conv_taps, att, logs, rows, halo
        )
    )


def solution(mesh):
    fine = Mesh(
        mesh.devices.reshape(4, 2, 4, 2, mesh.shape["fs"], mesh.shape["tp"]), SP + COLS
    )
    weights = P(SP, COLS)
    return jax.shard_map(
        body,
        mesh=fine,
        in_specs=(P(SP, None), P()) + (weights,) * 5 + (P(None, COLS), P(COLS)),
        out_specs=(P(SP, COLS), P(COLS, SP)),
        check_vma=False,
    )
```

```python
import functools

import jax
import jax.numpy as jnp
from jax import lax
from jax.experimental import pallas as pl
from jax.experimental.pallas import tpu as pltpu
from jax.sharding import Mesh, PartitionSpec as P


HEAD_DIM = 64
WINDOW = 128
EPS = 1e-06

SP = ("zh", "zl", "yh", "yl")
COLS = ("fs", "tp")
SIDE = 8
LANES = 128
RIM = 16
VMEM = pl.BlockSpec(memory_space=pltpu.VMEM)
SMEM = pl.BlockSpec(memory_space=pltpu.SMEM)
HBM = pl.BlockSpec(memory_space=pltpu.HBM)


def shift(value, dz, dy):
    pairs = []
    for z in range(SIDE):
        for y in range(SIDE):
            for core, sign in enumerate((1, -1)):
                to = (z + sign * dz) % SIDE * SIDE + (y + sign * dy) % SIDE
                pairs.append(((z * SIDE + y) * 2 + core, to * 2 + core))
    return lax.ppermute(value, SP + ("tp",), pairs)


def passed_along(value):
    n = SIDE * SIDE
    return lax.ppermute(value, SP, [(i, i + 1) for i in range(n - 1)])


def settings(mib):
    return pltpu.CompilerParams(vmem_limit_bytes=mib << 20)


def cost(us):
    return pl.CostEstimate(flops=int(us * 3.9e6), bytes_accessed=1 << 20, transcendentals=0)


def dot(a, b, dims=((1,), (0,))):
    return lax.dot_general(a, b, (dims, ((), ())), preferred_element_type=jnp.float32)


def column_sort():
    span = 2 * LANES
    row = lax.broadcasted_iota(jnp.int32, (span, span), 0)
    col = lax.broadcasted_iota(jnp.int32, (span, span), 1)
    target = ((row >> 5) & 1) * LANES + (row >> 6) * 32 + (row & 31)
    return (target == col).astype(jnp.bfloat16)


def norm_into(place, rows, gain, swap, out_ref):
    widened = rows.astype(jnp.float32)
    scale = lax.rsqrt(jnp.mean(widened * widened, axis=-1, keepdims=True) + EPS)
    normed = (widened * scale * gain).astype(jnp.bfloat16)
    span = 2 * LANES
    for zh in range(4):
        for zl in range(2):
            at = (zh * 2 + zl) * span
            sorted_cols = dot(normed[:, at : at + span], swap).astype(jnp.bfloat16)
            for yl in range(2):
                into = (place[0] ^ zl) * 2 + (place[1] ^ yl)
                out_ref[into, :, zh * LANES : (zh + 1) * LANES] = sorted_cols[
                    :, yl * LANES : (yl + 1) * LANES
                ]


def norm_kernel(place, tok_hbm, gain_ref, out_hbm, rim_ref, sem, *, block):
    n, width = tok_hbm.shape
    swap = column_sort()
    rim = pltpu.make_async_copy(tok_hbm.at[n - RIM : n, :], rim_ref, sem)
    rim.start()

    def step(tok_ref, out_ref):
        norm_into(place, tok_ref[...], gain_ref[...], swap, out_ref)

    pltpu.emit_pipeline(
        step,
        grid=(n // block,),
        in_specs=[pl.BlockSpec((block, width), lambda i: (i, 0))],
        out_specs=[pl.BlockSpec((4, block, width // 4), lambda i: (0, i, 0))],
    )(tok_hbm, out_hbm)
    rim.wait()


def norm_classes(place, rows, gain, block):
    n, width = rows.shape
    return pl.pallas_call(
        functools.partial(norm_kernel, block=block),
        in_specs=[SMEM, HBM, VMEM],
        out_specs=[HBM, VMEM],
        out_shape=[
            pltpu.HBM((4, n, width // 4), jnp.bfloat16),
            jax.ShapeDtypeStruct((RIM, width), jnp.bfloat16),
        ],
        scratch_shapes=[pltpu.SemaphoreType.DMA(())],
        compiler_params=settings(9),
        cost_estimate=cost(5),
        name="norm",
    )(place, rows, gain)


def key_copies(kv):
    left = lax.broadcasted_iota(jnp.int32, kv.shape, 1) < HEAD_DIM
    swapped = pltpu.roll(kv.astype(jnp.float32), HEAD_DIM, 1).astype(kv.dtype)
    zero = jnp.zeros_like(kv)
    return jnp.where(left, kv, zero), jnp.where(left, zero, swapped)


def attend_block(q, keys_lo, keys_hi, values, sinks, has_prev):
    q = q * jnp.asarray(HEAD_DIM ** (-0.5), q.dtype)
    keys = jnp.concatenate([keys_lo, keys_hi], axis=0)
    key_idx = lax.broadcasted_iota(jnp.int32, (WINDOW, WINDOW), 0)
    query_idx = lax.broadcasted_iota(jnp.int32, (WINDOW, WINDOW), 1)
    from_prev = key_idx > query_idx
    weights, logs = [], []
    for pair in range(2):
        both = dot(keys, q[:, pair * LANES : (pair + 1) * LANES], ((1,), (1,)))
        for side in range(2):
            head = pair * 2 + side
            prev = both[side * 256 : side * 256 + WINDOW]
            cur = both[side * 256 + WINDOW : side * 256 + 2 * WINDOW]
            if has_prev is not None:
                prev = jnp.where(has_prev, prev, -jnp.inf)
            scores = jnp.where(from_prev, prev, cur)
            top = jnp.maximum(jnp.max(scores, axis=0, keepdims=True), sinks[head])
            raised = jnp.exp(scores - top)
            total = jnp.sum(raised, axis=0, keepdims=True) + jnp.exp(sinks[head] - top)
            logs.append(top + jnp.log(total))
            share = raised * (1.0 / total)
            zero = jnp.zeros_like(share)
            weights.append(
                jnp.concatenate(
                    [jnp.where(from_prev, share, zero), jnp.where(from_prev, zero, share)], axis=0
                ).astype(jnp.bfloat16)
            )
    outs = []
    for pair in range(2):
        got = dot(values, jnp.concatenate(weights[pair * 2 : pair * 2 + 2], axis=1), ((0,), (0,)))
        stacked = jnp.concatenate([got[HEAD_DIM:, :WINDOW], got[HEAD_DIM:, WINDOW:]], axis=0)
        outs.append(stacked.T)
    return jnp.concatenate(outs, axis=1), jnp.concatenate(logs, axis=0)


def cut_kernel(own_ref, a_ref, b_ref):
    cols = a_ref.shape[1]
    a_ref[...] = own_ref[:, :cols]
    b_ref[...] = own_ref[:, cols:]


def cut_columns(own, cols):
    n, width = own.shape
    return pl.pallas_call(
        cut_kernel,
        in_specs=[VMEM],
        out_specs=[VMEM] * 2,
        out_shape=[
            jax.ShapeDtypeStruct((n, cols), own.dtype),
            jax.ShapeDtypeStruct((n, width - cols), own.dtype),
        ],
        compiler_params=settings(2),
        cost_estimate=cost(1),
        name="cut",
    )(own)


def early_kernel(x_hbm, own_ref, y_ref, sum_a, sum_b, x_ref, sems):
    n = x_ref.shape[1]
    cols = sum_a.shape[1]
    step = 256
    copies = []
    for k, at in enumerate(range(0, n, step)):
        copies.append(
            pltpu.make_async_copy(
                x_hbm.at[:, at : at + step, :], x_ref.at[:, at : at + step, :], sems.at[k]
            )
        )
        copies[-1].start()
    for k, at in enumerate(range(0, n, step)):
        copies[k].wait()
        mine = x_ref[0, at : at + step, :]
        sum_a[at : at + step, :] = dot(mine, own_ref[:, :cols]) + dot(
            x_ref[1, at : at + step, :], y_ref[...]
        )
        sum_b[at : at + step, :] = dot(mine, own_ref[:, cols:])


def early_sums(x, own, along_y):
    n = x.shape[1]
    cols = along_y.shape[1]
    return pl.pallas_call(
        early_kernel,
        in_specs=[HBM] + [VMEM] * 2,
        out_specs=[VMEM] * 3,
        out_shape=[
            jax.ShapeDtypeStruct((n, cols), jnp.float32),
            jax.ShapeDtypeStruct((n, own.shape[1] - cols), jnp.float32),
            jax.ShapeDtypeStruct(x.shape, x.dtype),
        ],
        scratch_shapes=[pltpu.SemaphoreType.DMA((n // 256,))],
        compiler_params=settings(4),
        cost_estimate=cost(3),
        name="early",
    )(x, own, along_y)


def tail_kernel(x_ref, sum_ref, w2, w3, rim_ref, out_ref):
    acc = sum_ref[...] + dot(x_ref[2], w2[...]) + dot(x_ref[3], w3[...])
    out_ref[:WINDOW, :] = acc.astype(jnp.bfloat16)
    for k in range(rim_ref.shape[1] // LANES):
        out_ref[WINDOW + k * RIM : WINDOW + (k + 1) * RIM, :] = rim_ref[
            :, k * LANES : (k + 1) * LANES
        ]


def tail_rows(x, sums, parts, rim):
    n, depth = x.shape[1], x.shape[2]
    last = n // WINDOW - 1
    rows = WINDOW + rim.shape[1] // LANES * RIM
    return pl.pallas_call(
        tail_kernel,
        grid=(1,),
        in_specs=[
            pl.BlockSpec((4, WINDOW, depth), lambda i: (0, last, 0)),
            pl.BlockSpec((WINDOW, LANES), lambda i: (last, 0)),
        ]
        + [pl.BlockSpec((depth, LANES), lambda i: (0, 0))] * 2
        + [pl.BlockSpec(rim.shape, lambda i: (0, 0))],
        out_specs=pl.BlockSpec((rows, LANES), lambda i: (0, 0)),
        out_shape=jax.ShapeDtypeStruct((rows, LANES), jnp.bfloat16),
        compiler_params=settings(3),
        cost_estimate=cost(1),
        name="tail",
    )(x, sums, *parts, rim)


def attn_kernel(sinks, x_ref, sum_ref, w2, w3, att_ref, log_ref, rows_ref, lo_ref, hi_ref):
    n = x_ref.shape[1]
    step = 256
    cols = rows_ref.shape[1]
    for at in range(0, n, step):
        acc = sum_ref[at : at + step, :] + dot(x_ref[2, at : at + step, :], w2[...])
        acc = acc + dot(x_ref[3, at : at + step, :], w3[:, :cols])
        rows = acc.astype(jnp.bfloat16)
        rows_ref[at : at + step, :] = rows
        lo_ref[at : at + step, :], hi_ref[at : at + step, :] = key_copies(rows[:, :LANES])
    heads = [sinks[h] for h in range(4)]
    att_ref[:WINDOW, :] = jnp.zeros((WINDOW, 2 * LANES), jnp.float32)
    log_ref[:, :WINDOW] = jnp.zeros((4, WINDOW), jnp.float32)

    for b in range(1, n // WINDOW):
        here, before = b * WINDOW, (b - 1) * WINDOW
        att, logs = attend_block(
            rows_ref[here : here + WINDOW, LANES:],
            lo_ref[before : here + WINDOW, :],
            hi_ref[before : here + WINDOW, :],
            rows_ref[before : here + WINDOW, :LANES],
            heads,
            None,
        )
        att_ref[here : here + WINDOW, :] = att
        log_ref[:, here : here + WINDOW] = logs


def attention(sinks, x, sums, parts):
    n = x.shape[1]
    cols = sums.shape[1]
    return pl.pallas_call(
        attn_kernel,
        in_specs=[SMEM] + [VMEM] * 4,
        out_specs=[VMEM] * 3,
        out_shape=[
            jax.ShapeDtypeStruct((n, 2 * LANES), jnp.float32),
            jax.ShapeDtypeStruct((4, n), jnp.float32),
            jax.ShapeDtypeStruct((n, cols), jnp.bfloat16),
        ],
        scratch_shapes=[pltpu.VMEM((n, LANES), jnp.bfloat16)] * 2,
        compiler_params=settings(8),
        cost_estimate=cost(8),
        name="attn",
    )(sinks, x, sums, *parts)


def conv_kernel(
    sinks, place, x_ref, sum_ref, w0, w1, w2, w3, gain_ref, taps_ref, att_ref, log_ref, rows_ref, halo_ref,
    out_hbm, log_hbm, out_ref, log_out, pad_ref, prev_x, sems, log_sem,
):
    n = x_ref.shape[1]
    width = 2 * LANES
    step = 256
    parts = [w[:, w.shape[1] - 2 * width :] for w in (w0, w1, w2, w3)]
    rim = [
        halo_ref[WINDOW + k * RIM : WINDOW + (k + 1) * RIM, :]
        for k in range(gain_ref.shape[1] // LANES)
    ]
    norm_into(place, jnp.concatenate(rim, axis=1), gain_ref[...], column_sort(), prev_x)
    acc = dot(prev_x[0], parts[0][:, :width])
    for c in range(1, 4):
        acc = acc + dot(prev_x[c], parts[c][:, :width])
    pad_ref[:8, :] = acc[8:16].astype(jnp.bfloat16).astype(jnp.float32)
    span = jnp.concatenate([halo_ref[:WINDOW, :], rows_ref[:WINDOW, :LANES]], axis=0)
    att0, log0 = attend_block(
        rows_ref[:WINDOW, LANES:],
        *key_copies(span),
        span,
        [sinks[h] for h in range(4)],
        place[2] > 0,
    )
    log_out[...] = log_ref[...]
    log_out[:, :WINDOW] = log0
    log_copy = pltpu.make_async_copy(log_out, log_hbm, log_sem)
    log_copy.start()
    taps = taps_ref[...].astype(jnp.float32)
    copies = []
    for k, at in enumerate(range(0, n, step)):
        acc = sum_ref[at : at + step, :] + dot(x_ref[1, at : at + step, :], parts[1])
        for c in range(2, 4):
            acc = acc + dot(x_ref[c, at : at + step, :], parts[c])
        rounded = acc.astype(jnp.bfloat16).astype(jnp.float32)
        pad_ref[8 + at : 8 + at + step, :] = rounded[:, :width]
        total = taps[0:1] * pad_ref[6 + at : 6 + at + step, :]
        total = total + taps[1:2] * pad_ref[7 + at : 7 + at + step, :]
        total = total + taps[2:3] * rounded[:, :width]
        gated = rounded[:, width:] * total
        if at == 0:
            first = jnp.concatenate([att0, att_ref[WINDOW:step, :]], axis=0)
        else:
            first = att_ref[at : at + step, :]
        out_ref[at : at + step, :] = (first + gated).astype(jnp.bfloat16)
        copies.append(
            pltpu.make_async_copy(
                out_ref.at[at : at + step, :], out_hbm.at[at : at + step, :], sems.at[k]
            )
        )
        copies[-1].start()
    for copy in copies:
        copy.wait()
    log_copy.wait()


def convolution(sinks, place, x, sums, parts, gain, taps, att, logs, rows, halo):
    n = x.shape[1]
    return pl.pallas_call(
        conv_kernel,
        in_specs=[SMEM] * 2 + [VMEM] * 12,
        out_specs=[HBM, HBM],
        out_shape=[
            jax.ShapeDtypeStruct((n, 2 * LANES), jnp.bfloat16),
            jax.ShapeDtypeStruct((4, n), jnp.float32),
        ],
        scratch_shapes=[
            pltpu.VMEM((n, 2 * LANES), jnp.bfloat16),
            pltpu.VMEM((4, n), jnp.float32),
            pltpu.VMEM((n + 8, 2 * LANES), jnp.float32),
            pltpu.VMEM((4, RIM, x.shape[2]), jnp.bfloat16),
            pltpu.SemaphoreType.DMA((n // 256,)),
            pltpu.SemaphoreType.DMA(()),
        ],
        compiler_params=settings(8),
        cost_estimate=cost(6),
        name="conv",
    )(sinks, place, x, sums, *parts, gain, taps, att, logs, rows, halo)


def body(
    tokens, norm_gain, w_query, w_key, w_value, w_conv_in, w_conv_gate, conv_taps, sink_logits
):
    return layer(
        tokens, norm_gain, (w_key, w_value, w_query), (w_conv_in, w_conv_gate), conv_taps, sink_logits
    )


def layer(tokens, norm_gain, attn_weights, conv_weights, conv_taps, sink_logits):
    _, width = tokens.shape
    gain = norm_gain.reshape(1, width)
    place = jnp.stack(
        [lax.axis_index("zl"), lax.axis_index("yl"), jnp.minimum(lax.axis_index(SP), 1)]
    ).astype(jnp.int32)

    mine = jnp.concatenate(attn_weights + conv_weights, axis=1)
    cut = sum(w.shape[1] for w in attn_weights)
    sent = jnp.broadcast_to(mine[None], (16,) + mine.shape)
    own = lax.all_to_all(sent, ("zh", "yh"), 0, 0)
    own = own.reshape(16 * mine.shape[0], mine.shape[1])

    corner = shift(own, -1, -1)

    def classes(block):
        along_y = shift(block, 0, 1)
        along_z = shift(block, 1, 0)
        return [own, along_y, along_z, corner]

    own_a, own_b = cut_columns(own, cut)
    parts_a = classes(own_a)
    parts_b = classes(own_b)
    near = pltpu.with_memory_space_constraint
    x_far, rim = norm_classes(place, near(tokens, pltpu.HBM), gain, 256)
    x_far = near(x_far, pltpu.HBM)
    sum_a, sum_b, x = early_sums(x_far, own, parts_a[1])
    last = tail_rows(x, sum_a, parts_a[2:], rim)
    halo = passed_along(last)
    att, logs, rows = attention(sink_logits, x, sum_a, parts_a[2:])
    return tuple(
        convolution(sink_logits, place, x, sum_b, parts_b, gain, conv_taps, att, logs, rows, halo)
    )


def solution(mesh):
    fine = Mesh(
        mesh.devices.reshape(4, 2, 4, 2, mesh.shape["fs"], mesh.shape["tp"]), SP + COLS
    )
    weights = P(SP, COLS)
    return jax.shard_map(
        body,
        mesh=fine,
        in_specs=(P(SP, None), P()) + (weights,) * 5 + (P(None, COLS), P(COLS)),
        out_specs=(P(SP, COLS), P(COLS, SP)),
        check_vma=False,
    )
```

```python
import jax
import jax.numpy as jnp
from jax import lax
from jax.experimental import pallas as pl
from jax.experimental.pallas import tpu as pltpu
from jax.sharding import Mesh, PartitionSpec as P


HEAD_DIM = 64
WINDOW = 128
EPS = 1e-06

SP = ("zh", "zl", "yh", "yl")
COLS = ("fs", "tp")
SIDE = 8
LANES = 128
RIM = 16
VMEM = pl.BlockSpec(memory_space=pltpu.VMEM)
SMEM = pl.BlockSpec(memory_space=pltpu.SMEM)
HBM = pl.BlockSpec(memory_space=pltpu.HBM)


def shift(value, dz, dy):
    pairs = []
    for z in range(SIDE):
        for y in range(SIDE):
            pairs.append((z * SIDE + y, (z + dz) % SIDE * SIDE + (y + dy) % SIDE))
    return lax.ppermute(value, SP, pairs)


def passed_along(value):
    n = SIDE * SIDE
    return lax.ppermute(value, SP, [(i, i + 1) for i in range(n - 1)])


def settings(mib):
    return pltpu.CompilerParams(vmem_limit_bytes=mib << 20)


def cost(us):
    return pl.CostEstimate(flops=int(us * 3.9e6), bytes_accessed=1 << 20, transcendentals=0)


def dot(a, b, dims=((1,), (0,))):
    return lax.dot_general(a, b, (dims, ((), ())), preferred_element_type=jnp.float32)


def column_sort():
    span = 2 * LANES
    row = lax.broadcasted_iota(jnp.int32, (span, span), 0)
    col = lax.broadcasted_iota(jnp.int32, (span, span), 1)
    target = ((row >> 5) & 1) * LANES + (row >> 6) * 32 + (row & 31)
    return (target == col).astype(jnp.bfloat16)


def norm_into(place, rows, gain, swap, out_ref):
    widened = rows.astype(jnp.float32)
    scale = lax.rsqrt(jnp.mean(widened * widened, axis=-1, keepdims=True) + EPS)
    normed = (widened * scale * gain).astype(jnp.bfloat16)
    span = 2 * LANES
    for zh in range(4):
        for zl in range(2):
            at = (zh * 2 + zl) * span
            sorted_cols = dot(normed[:, at : at + span], swap).astype(jnp.bfloat16)
            for yl in range(2):
                into = (place[0] ^ zl) * 2 + (place[1] ^ yl)
                out_ref[into, :, zh * LANES : (zh + 1) * LANES] = sorted_cols[
                    :, yl * LANES : (yl + 1) * LANES
                ]


def norm_kernel(place, tok_ref, gain_ref, out_ref, rim_ref):
    rim_ref[...] = tok_ref[tok_ref.shape[0] - RIM :, :]
    norm_into(place, tok_ref[...], gain_ref[...], column_sort(), out_ref)


def norm_classes(place, rows, gain, block):
    n, width = rows.shape
    return pl.pallas_call(
        norm_kernel,
        grid_spec=pltpu.PrefetchScalarGridSpec(
            num_scalar_prefetch=1,
            grid=(n // block,),
            in_specs=[
                pl.BlockSpec((block, width), lambda i, p: (i, 0)),
                pl.BlockSpec((1, width), lambda i, p: (0, 0)),
            ],
            out_specs=[
                pl.BlockSpec((4, block, width // 4), lambda i, p: (0, i, 0)),
                pl.BlockSpec((RIM, width), lambda i, p: (0, 0)),
            ],
        ),
        out_shape=[
            jax.ShapeDtypeStruct((4, n, width // 4), jnp.bfloat16),
            jax.ShapeDtypeStruct((RIM, width), jnp.bfloat16),
        ],
        compiler_params=settings(9),
        cost_estimate=cost(5),
        name="norm",
    )(place, rows, gain)


def key_copies(kv):
    left = lax.broadcasted_iota(jnp.int32, kv.shape, 1) < HEAD_DIM
    swapped = pltpu.roll(kv.astype(jnp.float32), HEAD_DIM, 1).astype(kv.dtype)
    zero = jnp.zeros_like(kv)
    return jnp.where(left, kv, zero), jnp.where(left, zero, swapped)


def attend_block(q, keys_lo, keys_hi, values, sinks, has_prev):
    q = q * jnp.asarray(HEAD_DIM ** (-0.5), q.dtype)
    keys = jnp.concatenate([keys_lo, keys_hi], axis=0)
    key_idx = lax.broadcasted_iota(jnp.int32, (WINDOW, WINDOW), 0)
    query_idx = lax.broadcasted_iota(jnp.int32, (WINDOW, WINDOW), 1)
    from_prev = key_idx > query_idx
    weights, scales, logs = [], [], []
    for pair in range(2):
        both = dot(keys, q[:, pair * LANES : (pair + 1) * LANES], ((1,), (1,)))
        for side in range(2):
            head = pair * 2 + side
            prev = both[side * 256 : side * 256 + WINDOW]
            cur = both[side * 256 + WINDOW : side * 256 + 2 * WINDOW]
            if has_prev is not None:
                prev = jnp.where(has_prev, prev, -jnp.inf)
            scores = jnp.where(from_prev, prev, cur)
            top = jnp.maximum(jnp.max(scores, axis=0, keepdims=True), sinks[head])
            raised = jnp.exp(scores - top)
            total = jnp.sum(raised, axis=0, keepdims=True) + jnp.exp(sinks[head] - top)
            logs.append(top + jnp.log(total))
            scales.append(1.0 / total)
            zero = jnp.zeros_like(raised)
            weights.append(
                jnp.concatenate(
                    [jnp.where(from_prev, raised, zero), jnp.where(from_prev, zero, raised)], axis=0
                ).astype(jnp.bfloat16)
            )
    outs = []
    for pair in range(2):
        got = dot(values, jnp.concatenate(weights[pair * 2 : pair * 2 + 2], axis=1), ((0,), (0,)))
        stacked = jnp.concatenate(
            [
                got[HEAD_DIM:, :WINDOW] * scales[pair * 2],
                got[HEAD_DIM:, WINDOW:] * scales[pair * 2 + 1],
            ],
            axis=0,
        )
        outs.append(stacked.T)
    return jnp.concatenate(outs, axis=1), jnp.concatenate(logs, axis=0)


def cut_kernel(own_ref, a_ref, b_ref):
    cols = a_ref.shape[1]
    a_ref[...] = own_ref[:, :cols]
    b_ref[...] = own_ref[:, cols:]


def cut_columns(own, cols):
    n, width = own.shape
    return pl.pallas_call(
        cut_kernel,
        in_specs=[VMEM],
        out_specs=[VMEM] * 2,
        out_shape=[
            jax.ShapeDtypeStruct((n, cols), own.dtype),
            jax.ShapeDtypeStruct((n, width - cols), own.dtype),
        ],
        compiler_params=settings(2),
        cost_estimate=cost(1),
        name="cut",
    )(own)


def early_kernel(x_ref, own_ref, y_ref, sum_a, sum_b):
    n = x_ref.shape[1]
    cols = sum_a.shape[1]
    step = 256
    for at in range(0, n, step):
        mine = x_ref[0, at : at + step, :]
        sum_a[at : at + step, :] = dot(mine, own_ref[:, :cols]) + dot(
            x_ref[1, at : at + step, :], y_ref[...]
        )
        sum_b[at : at + step, :] = dot(mine, own_ref[:, cols:])


def early_sums(x, own, along_y):
    n = x.shape[1]
    cols = along_y.shape[1]
    return pl.pallas_call(
        early_kernel,
        in_specs=[VMEM] * 3,
        out_specs=[VMEM] * 2,
        out_shape=[
            jax.ShapeDtypeStruct((n, cols), jnp.float32),
            jax.ShapeDtypeStruct((n, own.shape[1] - cols), jnp.float32),
        ],
        compiler_params=settings(4),
        cost_estimate=cost(2),
        name="early",
    )(x, own, along_y)


def tail_kernel(x_ref, sum_ref, w2, w3, rim_ref, out_ref):
    acc = sum_ref[...] + dot(x_ref[2], w2[...]) + dot(x_ref[3], w3[...])
    out_ref[:WINDOW, :] = acc.astype(jnp.bfloat16)
    for k in range(rim_ref.shape[1] // LANES):
        out_ref[WINDOW + k * RIM : WINDOW + (k + 1) * RIM, :] = rim_ref[
            :, k * LANES : (k + 1) * LANES
        ]


def tail_rows(x, sums, parts, rim):
    n, depth = x.shape[1], x.shape[2]
    last = n // WINDOW - 1
    rows = WINDOW + rim.shape[1] // LANES * RIM
    return pl.pallas_call(
        tail_kernel,
        grid=(1,),
        in_specs=[
            pl.BlockSpec((4, WINDOW, depth), lambda i: (0, last, 0)),
            pl.BlockSpec((WINDOW, LANES), lambda i: (last, 0)),
        ]
        + [pl.BlockSpec((depth, LANES), lambda i: (0, 0))] * 2
        + [pl.BlockSpec(rim.shape, lambda i: (0, 0))],
        out_specs=pl.BlockSpec((rows, LANES), lambda i: (0, 0)),
        out_shape=jax.ShapeDtypeStruct((rows, LANES), jnp.bfloat16),
        compiler_params=settings(3),
        cost_estimate=cost(1),
        name="tail",
    )(x, sums, *parts, rim)


def attn_kernel(sinks, x_ref, sum_ref, w2, w3, att_ref, log_ref, rows_ref, lo_ref, hi_ref):
    n = x_ref.shape[1]
    step = 256
    cols = rows_ref.shape[1]
    for at in range(0, n, step):
        acc = sum_ref[at : at + step, :] + dot(x_ref[2, at : at + step, :], w2[...])
        acc = acc + dot(x_ref[3, at : at + step, :], w3[:, :cols])
        rows = acc.astype(jnp.bfloat16)
        rows_ref[at : at + step, :] = rows
        lo_ref[at : at + step, :], hi_ref[at : at + step, :] = key_copies(rows[:, :LANES])
    heads = [sinks[h] for h in range(4)]
    att_ref[:WINDOW, :] = jnp.zeros((WINDOW, 2 * LANES), jnp.float32)
    log_ref[:, :WINDOW] = jnp.zeros((4, WINDOW), jnp.float32)

    for b in range(1, n // WINDOW):
        here, before = b * WINDOW, (b - 1) * WINDOW
        att, logs = attend_block(
            rows_ref[here : here + WINDOW, LANES:],
            lo_ref[before : here + WINDOW, :],
            hi_ref[before : here + WINDOW, :],
            rows_ref[before : here + WINDOW, :LANES],
            heads,
            None,
        )
        att_ref[here : here + WINDOW, :] = att
        log_ref[:, here : here + WINDOW] = logs


def attention(sinks, x, sums, parts):
    n = x.shape[1]
    cols = sums.shape[1]
    return pl.pallas_call(
        attn_kernel,
        in_specs=[SMEM] + [VMEM] * 4,
        out_specs=[VMEM] * 3,
        out_shape=[
            jax.ShapeDtypeStruct((n, 2 * LANES), jnp.float32),
            jax.ShapeDtypeStruct((4, n), jnp.float32),
            jax.ShapeDtypeStruct((n, cols), jnp.bfloat16),
        ],
        scratch_shapes=[pltpu.VMEM((n, LANES), jnp.bfloat16)] * 2,
        compiler_params=settings(8),
        cost_estimate=cost(8),
        name="attn",
    )(sinks, x, sums, *parts)


def conv_kernel(
    sinks, place, x_ref, sum_ref, w0, w1, w2, w3, gain_ref, taps_ref, att_ref, log_ref, rows_ref, halo_ref,
    out_hbm, log_hbm, out_ref, log_out, pad_ref, prev_x, sems, log_sem,
):
    n = x_ref.shape[1]
    width = 2 * LANES
    step = 256
    parts = [w[:, w.shape[1] - 2 * width :] for w in (w0, w1, w2, w3)]
    rim = [
        halo_ref[WINDOW + k * RIM : WINDOW + (k + 1) * RIM, :]
        for k in range(gain_ref.shape[1] // LANES)
    ]
    norm_into(place, jnp.concatenate(rim, axis=1), gain_ref[...], column_sort(), prev_x)
    acc = dot(prev_x[0], parts[0][:, :width])
    for c in range(1, 4):
        acc = acc + dot(prev_x[c], parts[c][:, :width])
    pad_ref[:8, :] = acc[8:16].astype(jnp.bfloat16).astype(jnp.float32)
    span = jnp.concatenate([halo_ref[:WINDOW, :], rows_ref[:WINDOW, :LANES]], axis=0)
    att0, log0 = attend_block(
        rows_ref[:WINDOW, LANES:],
        *key_copies(span),
        span,
        [sinks[h] for h in range(4)],
        place[2] > 0,
    )
    log_out[...] = log_ref[...]
    log_out[:, :WINDOW] = log0
    log_copy = pltpu.make_async_copy(log_out, log_hbm, log_sem)
    log_copy.start()
    taps = taps_ref[...].astype(jnp.float32)
    copies = []
    for k, at in enumerate(range(0, n, step)):
        acc = sum_ref[at : at + step, :] + dot(x_ref[1, at : at + step, :], parts[1])
        for c in range(2, 4):
            acc = acc + dot(x_ref[c, at : at + step, :], parts[c])
        rounded = acc.astype(jnp.bfloat16).astype(jnp.float32)
        pad_ref[8 + at : 8 + at + step, :] = rounded[:, :width]
        total = taps[0:1] * pad_ref[6 + at : 6 + at + step, :]
        total = total + taps[1:2] * pad_ref[7 + at : 7 + at + step, :]
        total = total + taps[2:3] * rounded[:, :width]
        gated = rounded[:, width:] * total
        if at == 0:
            first = jnp.concatenate([att0, att_ref[WINDOW:step, :]], axis=0)
        else:
            first = att_ref[at : at + step, :]
        out_ref[at : at + step, :] = (first + gated).astype(jnp.bfloat16)
        copies.append(
            pltpu.make_async_copy(
                out_ref.at[at : at + step, :], out_hbm.at[at : at + step, :], sems.at[k]
            )
        )
        copies[-1].start()
    for copy in copies:
        copy.wait()
    log_copy.wait()


def convolution(sinks, place, x, sums, parts, gain, taps, att, logs, rows, halo):
    n = x.shape[1]
    return pl.pallas_call(
        conv_kernel,
        in_specs=[SMEM] * 2 + [VMEM] * 12,
        out_specs=[HBM, HBM],
        out_shape=[
            jax.ShapeDtypeStruct((n, 2 * LANES), jnp.bfloat16),
            jax.ShapeDtypeStruct((4, n), jnp.float32),
        ],
        scratch_shapes=[
            pltpu.VMEM((n, 2 * LANES), jnp.bfloat16),
            pltpu.VMEM((4, n), jnp.float32),
            pltpu.VMEM((n + 8, 2 * LANES), jnp.float32),
            pltpu.VMEM((4, RIM, x.shape[2]), jnp.bfloat16),
            pltpu.SemaphoreType.DMA((n // 256,)),
            pltpu.SemaphoreType.DMA(()),
        ],
        compiler_params=settings(8),
        cost_estimate=cost(6),
        name="conv",
    )(sinks, place, x, sums, *parts, gain, taps, att, logs, rows, halo)


def body(
    tokens, norm_gain, w_query, w_key, w_value, w_conv_in, w_conv_gate, conv_taps, sink_logits
):
    return layer(
        tokens, norm_gain, (w_key, w_value, w_query), (w_conv_in, w_conv_gate), conv_taps, sink_logits
    )


def layer(tokens, norm_gain, attn_weights, conv_weights, conv_taps, sink_logits):
    _, width = tokens.shape
    gain = norm_gain.reshape(1, width)
    place = jnp.stack(
        [lax.axis_index("zl"), lax.axis_index("yl"), jnp.minimum(lax.axis_index(SP), 1)]
    ).astype(jnp.int32)

    mine = jnp.concatenate(attn_weights + conv_weights, axis=1)
    cut = sum(w.shape[1] for w in attn_weights)
    sent = jnp.broadcast_to(mine[None], (16,) + mine.shape)
    own = lax.all_to_all(sent, ("zh", "yh"), 0, 0)
    own = own.reshape(16 * mine.shape[0], mine.shape[1])

    corner = shift(own, -1, -1)

    def classes(block):
        along_y = shift(block, 0, 1)
        along_z = shift(block, 1, 0)
        return [own, along_y, along_z, corner]

    own_a, own_b = cut_columns(own, cut)
    parts_a = classes(own_a)
    parts_b = classes(own_b)
    near = pltpu.with_memory_space_constraint
    x, rim = norm_classes(place, near(tokens, pltpu.HBM), near(gain, pltpu.HBM), 256)
    sum_a, sum_b = early_sums(x, own, parts_a[1])
    last = tail_rows(x, sum_a, parts_a[2:], rim)
    halo = passed_along(last)
    att, logs, rows = attention(sink_logits, x, sum_a, parts_a[2:])
    return tuple(
        convolution(sink_logits, place, x, sum_b, parts_b, gain, conv_taps, att, logs, rows, halo)
    )


def solution(mesh):
    fine = Mesh(
        mesh.devices.reshape(4, 2, 4, 2, mesh.shape["fs"], mesh.shape["tp"]), SP + COLS
    )
    weights = P(SP, COLS)
    return jax.shard_map(
        body,
        mesh=fine,
        in_specs=(P(SP, None), P()) + (weights,) * 5 + (P(None, COLS), P(COLS)),
        out_specs=(P(SP, COLS), P(COLS, SP)),
        check_vma=False,
    )
```

```python
import jax
import jax.numpy as jnp
from jax import lax
from jax.experimental import pallas as pl
from jax.experimental.pallas import tpu as pltpu
from jax.sharding import Mesh, PartitionSpec as P


HEAD_DIM = 64
WINDOW = 128
EPS = 1e-06

SP = ("zh", "zl", "yh", "yl")
COLS = ("fs", "tp")
SIDE = 8
LANES = 128
RIM = 8
VMEM = pl.BlockSpec(memory_space=pltpu.VMEM)
SMEM = pl.BlockSpec(memory_space=pltpu.SMEM)
HBM = pl.BlockSpec(memory_space=pltpu.HBM)


def shift(value, dz, dy):
    pairs = []
    for z in range(SIDE):
        for y in range(SIDE):
            pairs.append((z * SIDE + y, (z + dz) % SIDE * SIDE + (y + dy) % SIDE))
    return lax.ppermute(value, SP, pairs)


def passed_along(value):
    n = SIDE * SIDE
    return lax.ppermute(value, SP, [(i, i + 1) for i in range(n - 1)])


def settings(mib):
    return pltpu.CompilerParams(vmem_limit_bytes=mib << 20)


def cost(us):
    return pl.CostEstimate(flops=int(us * 3.9e6), bytes_accessed=1 << 20, transcendentals=0)


def dot(a, b, dims=((1,), (0,))):
    return lax.dot_general(a, b, (dims, ((), ())), preferred_element_type=jnp.float32)


def column_sort():
    span = 2 * LANES
    row = lax.broadcasted_iota(jnp.int32, (span, span), 0)
    col = lax.broadcasted_iota(jnp.int32, (span, span), 1)
    target = ((row >> 5) & 1) * LANES + (row >> 6) * 32 + (row & 31)
    return (target == col).astype(jnp.bfloat16)


def norm_into(place, rows, gain, swap, out_ref):
    widened = rows.astype(jnp.float32)
    scale = lax.rsqrt(jnp.mean(widened * widened, axis=-1, keepdims=True) + EPS)
    normed = (widened * scale * gain).astype(jnp.bfloat16)
    span = 2 * LANES
    for zh in range(4):
        for zl in range(2):
            at = (zh * 2 + zl) * span
            sorted_cols = dot(normed[:, at : at + span], swap).astype(jnp.bfloat16)
            for yl in range(2):
                into = (place[0] ^ zl) * 2 + (place[1] ^ yl)
                out_ref[into, :, zh * LANES : (zh + 1) * LANES] = sorted_cols[
                    :, yl * LANES : (yl + 1) * LANES
                ]


def norm_kernel(place, tok_ref, gain_ref, out_ref, rim_ref):
    rim_ref[...] = tok_ref[tok_ref.shape[0] - RIM :, :]
    norm_into(place, tok_ref[...], gain_ref[...], column_sort(), out_ref)


def norm_classes(place, rows, gain, block):
    n, width = rows.shape
    return pl.pallas_call(
        norm_kernel,
        grid_spec=pltpu.PrefetchScalarGridSpec(
            num_scalar_prefetch=1,
            grid=(n // block,),
            in_specs=[
                pl.BlockSpec((block, width), lambda i, p: (i, 0)),
                pl.BlockSpec((1, width), lambda i, p: (0, 0)),
            ],
            out_specs=[
                pl.BlockSpec((4, block, width // 4), lambda i, p: (0, i, 0)),
                pl.BlockSpec((RIM, width), lambda i, p: (0, 0)),
            ],
        ),
        out_shape=[
            jax.ShapeDtypeStruct((4, n, width // 4), jnp.bfloat16),
            jax.ShapeDtypeStruct((RIM, width), jnp.bfloat16),
        ],
        compiler_params=settings(9),
        cost_estimate=cost(5),
        name="norm",
    )(place, rows, gain)


def key_copies(kv):
    left = lax.broadcasted_iota(jnp.int32, kv.shape, 1) < HEAD_DIM
    swapped = pltpu.roll(kv.astype(jnp.float32), HEAD_DIM, 1).astype(kv.dtype)
    zero = jnp.zeros_like(kv)
    return jnp.where(left, kv, zero), jnp.where(left, zero, swapped)


def attend_block(q, keys_lo, keys_hi, values, sinks, has_prev):
    q = q * jnp.asarray(HEAD_DIM ** (-0.5), q.dtype)
    keys = jnp.concatenate([keys_lo, keys_hi], axis=0)
    key_idx = lax.broadcasted_iota(jnp.int32, (WINDOW, WINDOW), 0)
    query_idx = lax.broadcasted_iota(jnp.int32, (WINDOW, WINDOW), 1)
    from_prev = key_idx > query_idx
    weights, logs = [], []
    for pair in range(2):
        both = dot(keys, q[:, pair * LANES : (pair + 1) * LANES], ((1,), (1,)))
        for side in range(2):
            head = pair * 2 + side
            prev = both[side * 256 : side * 256 + WINDOW]
            cur = both[side * 256 + WINDOW : side * 256 + 2 * WINDOW]
            if has_prev is not None:
                prev = jnp.where(has_prev, prev, -jnp.inf)
            scores = jnp.where(from_prev, prev, cur)
            top = jnp.maximum(jnp.max(scores, axis=0, keepdims=True), sinks[head])
            raised = jnp.exp(scores - top)
            total = jnp.sum(raised, axis=0, keepdims=True) + jnp.exp(sinks[head] - top)
            logs.append(top + jnp.log(total))
            share = raised * (1.0 / total)
            zero = jnp.zeros_like(share)
            weights.append(
                jnp.concatenate(
                    [jnp.where(from_prev, share, zero), jnp.where(from_prev, zero, share)], axis=0
                ).astype(jnp.bfloat16)
            )
    outs = []
    for pair in range(2):
        got = dot(values, jnp.concatenate(weights[pair * 2 : pair * 2 + 2], axis=1), ((0,), (0,)))
        stacked = jnp.concatenate([got[HEAD_DIM:, :WINDOW], got[HEAD_DIM:, WINDOW:]], axis=0)
        outs.append(stacked.T)
    return jnp.concatenate(outs, axis=1), jnp.concatenate(logs, axis=0)


def cut_kernel(own_ref, a_ref, b_ref):
    cols = a_ref.shape[1]
    a_ref[...] = own_ref[:, :cols]
    b_ref[...] = own_ref[:, cols:]


def cut_columns(own, cols):
    n, width = own.shape
    return pl.pallas_call(
        cut_kernel,
        in_specs=[VMEM],
        out_specs=[VMEM] * 2,
        out_shape=[
            jax.ShapeDtypeStruct((n, cols), own.dtype),
            jax.ShapeDtypeStruct((n, width - cols), own.dtype),
        ],
        compiler_params=settings(2),
        cost_estimate=cost(1),
        name="cut",
    )(own)


def early_kernel(x_ref, own_ref, y_ref, sum_a, sum_b):
    n = x_ref.shape[1]
    cols = sum_a.shape[1]
    step = 256
    for at in range(0, n, step):
        mine = x_ref[0, at : at + step, :]
        sum_a[at : at + step, :] = dot(mine, own_ref[:, :cols]) + dot(
            x_ref[1, at : at + step, :], y_ref[...]
        )
        sum_b[at : at + step, :] = dot(mine, own_ref[:, cols:])


def early_sums(x, own, along_y):
    n = x.shape[1]
    cols = along_y.shape[1]
    return pl.pallas_call(
        early_kernel,
        in_specs=[VMEM] * 3,
        out_specs=[VMEM] * 2,
        out_shape=[
            jax.ShapeDtypeStruct((n, cols), jnp.float32),
            jax.ShapeDtypeStruct((n, own.shape[1] - cols), jnp.float32),
        ],
        compiler_params=settings(4),
        cost_estimate=cost(2),
        name="early",
    )(x, own, along_y)


def tail_kernel(x_ref, sum_ref, w2, w3, rim_ref, out_ref):
    acc = sum_ref[...] + dot(x_ref[2], w2[...]) + dot(x_ref[3], w3[...])
    out_ref[:WINDOW, :] = acc.astype(jnp.bfloat16)
    for k in range(rim_ref.shape[1] // LANES):
        out_ref[WINDOW + k * RIM : WINDOW + (k + 1) * RIM, :] = rim_ref[
            :, k * LANES : (k + 1) * LANES
        ]


def tail_rows(x, sums, parts, rim):
    n, depth = x.shape[1], x.shape[2]
    last = n // WINDOW - 1
    rows = WINDOW + rim.shape[1] // LANES * RIM
    return pl.pallas_call(
        tail_kernel,
        grid=(1,),
        in_specs=[
            pl.BlockSpec((4, WINDOW, depth), lambda i: (0, last, 0)),
            pl.BlockSpec((WINDOW, LANES), lambda i: (last, 0)),
        ]
        + [pl.BlockSpec((depth, LANES), lambda i: (0, 0))] * 2
        + [pl.BlockSpec(rim.shape, lambda i: (0, 0))],
        out_specs=pl.BlockSpec((rows, LANES), lambda i: (0, 0)),
        out_shape=jax.ShapeDtypeStruct((rows, LANES), jnp.bfloat16),
        compiler_params=settings(3),
        cost_estimate=cost(1),
        name="tail",
    )(x, sums, *parts, rim)


def attn_kernel(sinks, x_ref, sum_ref, w2, w3, att_ref, log_ref, rows_ref, lo_ref, hi_ref):
    n = x_ref.shape[1]
    step = 256
    cols = rows_ref.shape[1]
    for at in range(0, n, step):
        acc = sum_ref[at : at + step, :] + dot(x_ref[2, at : at + step, :], w2[...])
        acc = acc + dot(x_ref[3, at : at + step, :], w3[:, :cols])
        rows = acc.astype(jnp.bfloat16)
        rows_ref[at : at + step, :] = rows
        lo_ref[at : at + step, :], hi_ref[at : at + step, :] = key_copies(rows[:, :LANES])
    heads = [sinks[h] for h in range(4)]
    att_ref[:WINDOW, :] = jnp.zeros((WINDOW, 2 * LANES), jnp.float32)
    log_ref[:, :WINDOW] = jnp.zeros((4, WINDOW), jnp.float32)

    for b in range(1, n // WINDOW):
        here, before = b * WINDOW, (b - 1) * WINDOW
        att, logs = attend_block(
            rows_ref[here : here + WINDOW, LANES:],
            lo_ref[before : here + WINDOW, :],
            hi_ref[before : here + WINDOW, :],
            rows_ref[before : here + WINDOW, :LANES],
            heads,
            None,
        )
        att_ref[here : here + WINDOW, :] = att
        log_ref[:, here : here + WINDOW] = logs


def attention(sinks, x, sums, parts):
    n = x.shape[1]
    cols = sums.shape[1]
    return pl.pallas_call(
        attn_kernel,
        in_specs=[SMEM] + [VMEM] * 4,
        out_specs=[VMEM] * 3,
        out_shape=[
            jax.ShapeDtypeStruct((n, 2 * LANES), jnp.float32),
            jax.ShapeDtypeStruct((4, n), jnp.float32),
            jax.ShapeDtypeStruct((n, cols), jnp.bfloat16),
        ],
        scratch_shapes=[pltpu.VMEM((n, LANES), jnp.bfloat16)] * 2,
        compiler_params=settings(8),
        cost_estimate=cost(8),
        name="attn",
    )(sinks, x, sums, *parts)


def conv_kernel(
    sinks, place, x_ref, sum_ref, w0, w1, w2, w3, gain_ref, taps_ref, att_ref, log_ref, rows_ref, halo_ref,
    out_hbm, log_hbm, out_ref, log_out, pad_ref, prev_x, sems, log_sem,
):
    n = x_ref.shape[1]
    width = 2 * LANES
    step = 256
    parts = [w[:, w.shape[1] - 2 * width :] for w in (w0, w1, w2, w3)]
    rim = [
        halo_ref[WINDOW + k * RIM : WINDOW + (k + 1) * RIM, :]
        for k in range(gain_ref.shape[1] // LANES)
    ]
    norm_into(place, jnp.concatenate(rim, axis=1), gain_ref[...], column_sort(), prev_x)
    acc = dot(prev_x[0], parts[0][:, :width])
    for c in range(1, 4):
        acc = acc + dot(prev_x[c], parts[c][:, :width])
    pad_ref[:8, :] = acc[RIM - 8 : RIM].astype(jnp.bfloat16).astype(jnp.float32)
    span = jnp.concatenate([halo_ref[:WINDOW, :], rows_ref[:WINDOW, :LANES]], axis=0)
    att0, log0 = attend_block(
        rows_ref[:WINDOW, LANES:],
        *key_copies(span),
        span,
        [sinks[h] for h in range(4)],
        place[2] > 0,
    )
    log_out[...] = log_ref[...]
    log_out[:, :WINDOW] = log0
    log_copy = pltpu.make_async_copy(log_out, log_hbm, log_sem)
    log_copy.start()
    taps = taps_ref[...].astype(jnp.float32)
    copies = []
    for k, at in enumerate(range(0, n, step)):
        acc = sum_ref[at : at + step, :] + dot(x_ref[1, at : at + step, :], parts[1])
        for c in range(2, 4):
            acc = acc + dot(x_ref[c, at : at + step, :], parts[c])
        rounded = acc.astype(jnp.bfloat16).astype(jnp.float32)
        pad_ref[8 + at : 8 + at + step, :] = rounded[:, :width]
        total = taps[0:1] * pad_ref[6 + at : 6 + at + step, :]
        total = total + taps[1:2] * pad_ref[7 + at : 7 + at + step, :]
        total = total + taps[2:3] * rounded[:, :width]
        gated = rounded[:, width:] * total
        if at == 0:
            first = jnp.concatenate([att0, att_ref[WINDOW:step, :]], axis=0)
        else:
            first = att_ref[at : at + step, :]
        out_ref[at : at + step, :] = (first + gated).astype(jnp.bfloat16)
        copies.append(
            pltpu.make_async_copy(
                out_ref.at[at : at + step, :], out_hbm.at[at : at + step, :], sems.at[k]
            )
        )
        copies[-1].start()
    for copy in copies:
        copy.wait()
    log_copy.wait()


def convolution(sinks, place, x, sums, parts, gain, taps, att, logs, rows, halo):
    n = x.shape[1]
    return pl.pallas_call(
        conv_kernel,
        in_specs=[SMEM] * 2 + [VMEM] * 12,
        out_specs=[HBM, HBM],
        out_shape=[
            jax.ShapeDtypeStruct((n, 2 * LANES), jnp.bfloat16),
            jax.ShapeDtypeStruct((4, n), jnp.float32),
        ],
        scratch_shapes=[
            pltpu.VMEM((n, 2 * LANES), jnp.bfloat16),
            pltpu.VMEM((4, n), jnp.float32),
            pltpu.VMEM((n + 8, 2 * LANES), jnp.float32),
            pltpu.VMEM((4, RIM, x.shape[2]), jnp.bfloat16),
            pltpu.SemaphoreType.DMA((n // 256,)),
            pltpu.SemaphoreType.DMA(()),
        ],
        compiler_params=settings(8),
        cost_estimate=cost(6),
        name="conv",
    )(sinks, place, x, sums, *parts, gain, taps, att, logs, rows, halo)


def body(
    tokens, norm_gain, w_query, w_key, w_value, w_conv_in, w_conv_gate, conv_taps, sink_logits
):
    return layer(
        tokens, norm_gain, (w_key, w_value, w_query), (w_conv_in, w_conv_gate), conv_taps, sink_logits
    )


def layer(tokens, norm_gain, attn_weights, conv_weights, conv_taps, sink_logits):
    _, width = tokens.shape
    gain = norm_gain.reshape(1, width)
    place = jnp.stack(
        [lax.axis_index("zl"), lax.axis_index("yl"), jnp.minimum(lax.axis_index(SP), 1)]
    ).astype(jnp.int32)

    mine = jnp.concatenate(attn_weights + conv_weights, axis=1)
    cut = sum(w.shape[1] for w in attn_weights)
    sent = jnp.broadcast_to(mine[None], (16,) + mine.shape)
    own = lax.all_to_all(sent, ("zh", "yh"), 0, 0)
    own = own.reshape(16 * mine.shape[0], mine.shape[1])

    corner = shift(own, -1, -1)

    def classes(block):
        along_y = shift(block, 0, 1)
        along_z = shift(block, 1, 0)
        return [own, along_y, along_z, corner]

    own_a, own_b = cut_columns(own, cut)
    parts_a = classes(own_a)
    parts_b = classes(own_b)
    near = pltpu.with_memory_space_constraint
    x, rim = norm_classes(place, near(tokens, pltpu.HBM), near(gain, pltpu.HBM), 256)
    sum_a, sum_b = early_sums(x, own, parts_a[1])
    last = tail_rows(x, sum_a, parts_a[2:], rim)
    halo = passed_along(last)
    att, logs, rows = attention(sink_logits, x, sum_a, parts_a[2:])
    return tuple(
        convolution(sink_logits, place, x, sum_b, parts_b, gain, conv_taps, att, logs, rows, halo)
    )


def solution(mesh):
    fine = Mesh(
        mesh.devices.reshape(4, 2, 4, 2, mesh.shape["fs"], mesh.shape["tp"]), SP + COLS
    )
    weights = P(SP, COLS)
    return jax.shard_map(
        body,
        mesh=fine,
        in_specs=(P(SP, None), P()) + (weights,) * 5 + (P(None, COLS), P(COLS)),
        out_specs=(P(SP, COLS), P(COLS, SP)),
        check_vma=False,
    )
```
